32 devices in a mesh: sp: 16 (over z, y, x), tp: 2 (over core).
Axes of the slice: x: 2, y: 2, z: 4, core: 2. Of those that a mesh axis runs over, the one named last changes fastest.
Arguments:
- queries: bfloat16 [8192, 2048], P('sp', 'tp'), may hold values from -14 to 14
- key_states: bfloat16 [8192, 512], P('sp', 'tp'), may hold values from -14 to 14
- value_states: bfloat16 [8192, 512], P('sp', 'tp'), may hold values from -6 to 6
- sink_logits: float32 [32], P('tp'), may hold values from 0 to 5
- out_weight: bfloat16 [2048, 2048], P('tp'), may hold values from -0.125 to 0.125
- residual: bfloat16 [8192, 2048], P(('sp', 'tp')), may hold values from -6 to 6
- gain_attn: float32 [2048], replicated, may hold values from 0.1 to 1.9
- gain_before: float32 [2048], replicated, may hold values from 0.1 to 1.9
- gain_after: float32 [2048], replicated, may hold values from 0.1 to 1.9
- gate_weight: bfloat16 [2048, 5632], P('sp', 'tp'), may hold values from -0.125 to 0.125
- value_weight: bfloat16 [2048, 5632], P('sp', 'tp'), may hold values from -0.125 to 0.125
- gate_taps: float32 [3, 5632], P(None, 'tp'), may hold values from -3 to 3
- value_taps: float32 [3, 5632], P(None, 'tp'), may hold values from -3 to 3
- down_weight: bfloat16 [5632, 2048], P('tp', 'sp'), may hold values from -0.078125 to 0.078125
Outputs:
- layer_out: bfloat16 [8192, 2048], P(('sp', 'tp'))
The draws below stay inside these ranges and needn't reach their ends.
All inputs are finite; a program needn't handle non-finite values.
Results may differ from the reference program's by a relative error of at most 0.018.
Values may be sent and summed in bfloat16 or wider, within the bound.
A program may use at most 128 MiB of HBM per device.

```python
import jax
import jax.numpy as jnp
from jax import lax

D = 2048
HQ = 32
KV = 8
HD = 64
FF = 5632
WINDOW = 128
CONVK = 3
TOKENS = 8192
N_TP = 2


def drawn_keys(key):
    base = jax.random.truncated_normal(jax.random.fold_in(key, 11), -2.5, 2.5, (TOKENS, KV * HD), jnp.float32)
    return base


def draw_key_states(key, part):
    base = drawn_keys(key)
    return base.astype(jnp.bfloat16)


def draw_queries(key, part):
    own = jax.random.truncated_normal(jax.random.fold_in(key, 21), -2.5, 2.5, (TOKENS, HQ * HD), jnp.float32)
    return own.astype(jnp.bfloat16)


def block_scale(key, shape, cuts, smallest, high):
    loudness, own = 1.0, jax.random.fold_in(key, 6)
    for axis_at, blocks in cuts:
        steps = jnp.exp(jax.random.uniform(jax.random.fold_in(own, axis_at), (blocks,), jnp.float32, smallest / len(cuts), high / len(cuts)))
        loudness = loudness * jnp.repeat(steps, shape[axis_at] // blocks).reshape([-1 if axis == axis_at else 1 for axis in range(len(shape))])
    return loudness


def scatter_about(rng, extent, scale, most, shards=(), kind=jnp.bfloat16):
    loudness = block_scale(rng, extent, shards, -0.22, 0.18) if shards else 1.0
    drawn = jax.random.normal(rng, extent, jnp.float32) * scale * loudness
    return jnp.minimum(jnp.maximum(drawn, -most), most).astype(kind)


def setup_inputs(seed: int = 0) -> dict:
    arg_keys = jax.random.split(jax.random.key(seed), 15)
    return {
        "queries": draw_queries(jax.random.fold_in(arg_keys[14], 71), 0),
        "key_states": draw_key_states(jax.random.fold_in(arg_keys[14], 71), 0),
        "value_states": scatter_about(arg_keys[2], (TOKENS, KV * HD), 1.0, 6.0, ((0, 16), (1, 2))),
        "sink_logits": jnp.clip(5.0 * jax.random.uniform(arg_keys[3], (HQ,), jnp.float32) ** block_scale(arg_keys[3], (HQ,), ((0, 2),), -0.2, 0.2), 0.0, 5.0),
        "out_weight": scatter_about(arg_keys[4], (HQ * HD, D), (HQ * HD) ** -0.5, 0.125, ((0, 2),)),
        "residual": scatter_about(arg_keys[5], (TOKENS, D), 1.0, 6.0, ((0, 32),)),
        "gain_attn": jnp.clip(1.0 + 0.18 * jax.random.normal(arg_keys[6], (D,), jnp.float32), 0.1, 1.9),
        "gain_before": jnp.clip(1.0 + 0.18 * jax.random.normal(arg_keys[7], (D,), jnp.float32), 0.1, 1.9),
        "gain_after": jnp.clip(1.0 + 0.18 * jax.random.normal(arg_keys[8], (D,), jnp.float32), 0.1, 1.9),
        "gate_weight": scatter_about(arg_keys[9], (D, FF), D ** -0.5, 0.125, ((0, 16), (1, 2))),
        "value_weight": scatter_about(arg_keys[10], (D, FF), D ** -0.5, 0.125, ((0, 16), (1, 2))),
        "gate_taps": scatter_about(arg_keys[11], (CONVK, FF), 0.577, 3.0, ((1, 2),), jnp.float32),
        "value_taps": scatter_about(arg_keys[12], (CONVK, FF), 0.577, 3.0, ((1, 2),), jnp.float32),
        "down_weight": scatter_about(arg_keys[13], (FF, D), FF ** -0.5, 0.078125, ((0, 2), (1, 16))),
    }


NEG_FILL = -1e+30

def rms_scale(matrix):
    return matrix * lax.rsqrt(lax.optimization_barrier(jnp.mean(matrix * matrix, axis=-1, keepdims=True)) + 1e-06)

def attention(queries, key_states, value_states, sink_logits):
    length = queries.shape[0]
    blocks = length // WINDOW
    grouping = HQ // KV
    zeros_rows = jnp.zeros((WINDOW, KV * HD), jnp.bfloat16)
    keys_ext = jnp.concatenate([zeros_rows, key_states], axis=0).reshape(blocks + 1, WINDOW, KV, HD)
    values_ext = jnp.concatenate([zeros_rows, value_states], axis=0).reshape(blocks + 1, WINDOW, KV, HD)
    key_blocks = jnp.concatenate([keys_ext[:-1], keys_ext[1:]], axis=1)
    value_blocks = jnp.concatenate([values_ext[:-1], values_ext[1:]], axis=1)
    query_blocks = queries.reshape(blocks, WINDOW, KV, grouping, HD)
    qpos = jnp.arange(length, dtype=jnp.int32).reshape(blocks, WINDOW)
    kpos = jnp.concatenate([qpos - WINDOW, qpos], axis=1)
    visible = (kpos[:, None, :] <= qpos[:, :, None]) & (qpos[:, :, None] - kpos[:, None, :] < WINDOW) & (kpos[:, None, :] >= 0)
    sinks_all = sink_logits.reshape(KV, grouping)

    def one_head(inputs):
        query_part, key_part, value_part, sink_part = inputs
        scores = jnp.einsum('nqgd,nkd->ngqk', query_part.astype(jnp.float32), key_part.astype(jnp.float32)) * HD ** (-0.5)
        scores = jnp.where(visible[:, None], scores, NEG_FILL)
        sink_col = sink_part[None, :, None]
        top = jnp.maximum(lax.optimization_barrier(jnp.max(scores, axis=-1)), sink_col)
        expo = jnp.exp(scores - top[..., None])
        total = lax.optimization_barrier(jnp.sum(expo, axis=-1)) + jnp.exp(sink_col - top)
        probs = (expo / total[..., None]).astype(jnp.bfloat16)
        result = jnp.einsum('ngqk,nkd->nqgd', probs.astype(jnp.float32), value_part.astype(jnp.float32))
        return result.astype(jnp.bfloat16)
    heads_out = lax.map(one_head, (jnp.moveaxis(query_blocks, 2, 0), jnp.moveaxis(key_blocks, 2, 0), jnp.moveaxis(value_blocks, 2, 0), sinks_all))
    return jnp.moveaxis(heads_out, 0, 2).reshape(length, HQ * HD)

def grouped_sum(left, right):
    width = left.shape[1] // N_TP
    total = jnp.zeros((left.shape[0], right.shape[1]), jnp.float32)
    for group_index in range(N_TP):
        part = jnp.dot(left[:, group_index * width:(group_index + 1) * width], right[group_index * width:(group_index + 1) * width], preferred_element_type=jnp.float32)
        total = total + part.astype(jnp.bfloat16).astype(jnp.float32)
    return total

def causal_taps(upward, kernel):
    length = upward.shape[0]
    padded = jnp.concatenate([jnp.zeros((CONVK - 1, upward.shape[1]), jnp.bfloat16), upward], axis=0).astype(jnp.float32)
    result = jnp.zeros((length, upward.shape[1]), jnp.float32)
    for tap_index in range(CONVK):
        result = result + kernel[tap_index][None, :] * padded[tap_index:tap_index + length]
    return result

def reference(queries, key_states, value_states, sink_logits, out_weight, residual, gain_attn, gain_before, gain_after, gate_weight, value_weight, gate_taps, value_taps, down_weight):
    attended = attention(queries, key_states, value_states, sink_logits)
    attn_proj = grouped_sum(attended, out_weight)
    middle = residual.astype(jnp.float32) + rms_scale(attn_proj) * gain_attn
    normed = (rms_scale(middle) * gain_before).astype(jnp.bfloat16)
    gate_up = jnp.dot(normed, gate_weight, preferred_element_type=jnp.float32).astype(jnp.bfloat16)
    value_up = jnp.dot(normed, value_weight, preferred_element_type=jnp.float32).astype(jnp.bfloat16)
    gate_conv = causal_taps(gate_up, gate_taps)
    value_conv = causal_taps(value_up, value_taps)
    hidden = (jax.nn.silu(gate_conv) * value_conv).astype(jnp.bfloat16)
    down = grouped_sum(hidden, down_weight)
    return (middle + rms_scale(down) * gain_after).astype(jnp.bfloat16)
```

```python
import functools

import jax
import jax.numpy as jnp
from jax import lax
from jax.experimental import pallas as pl
from jax.experimental.pallas import tpu as pltpu
from jax.sharding import PartitionSpec as P

HD = 64
WINDOW = 128
TEAM = 4


NEG_FILL = -1e30
MESH = pl.DeviceIdType.MESH
VMEM_BYTES = 63 * 1024 * 1024

def passed_along(block, axis, distance):
    devices = range(lax.axis_size(axis))
    route = [(i - distance, i) for i in devices if i - distance in devices]
    return lax.ppermute(block, axis, route)


def rms_scale(matrix):
    return matrix * lax.rsqrt(jnp.mean(matrix * matrix, axis=-1, keepdims=True) + 1e-06)


def attention_local(queries, key_states, value_states, sink_logits):
    length = queries.shape[0]
    blocks = length // WINDOW
    kv_local = key_states.shape[1] // HD
    grouping = queries.shape[1] // key_states.shape[1]
    earlier_keys, earlier_values = passed_along(
        (key_states[length - WINDOW :], value_states[length - WINDOW :]), "sp", 1
    )
    keys_ext = jnp.concatenate([earlier_keys, key_states], axis=0).reshape(
        blocks + 1, WINDOW, kv_local, HD
    )
    values_ext = jnp.concatenate([earlier_values, value_states], axis=0).reshape(
        blocks + 1, WINDOW, kv_local, HD
    )
    key_blocks = jnp.concatenate([keys_ext[:-1], keys_ext[1:]], axis=1)
    value_blocks = jnp.concatenate([values_ext[:-1], values_ext[1:]], axis=1)
    query_blocks = queries.reshape(blocks, WINDOW, kv_local, grouping, HD)
    offset = lax.axis_index("sp") * length
    qpos = (offset + jnp.arange(length, dtype=jnp.int32)).reshape(blocks, WINDOW)
    kpos = jnp.concatenate([qpos - WINDOW, qpos], axis=1)
    visible = (
        (kpos[:, None, :] <= qpos[:, :, None])
        & (qpos[:, :, None] - kpos[:, None, :] < WINDOW)
        & (kpos[:, None, :] >= 0)
    )
    scores = jnp.einsum(
        "nqhgd,nkhd->nhgqk", query_blocks, key_blocks, preferred_element_type=jnp.float32
    ) * HD ** (-0.5)
    scores = jnp.where(visible[:, None, None], scores, NEG_FILL)
    sink_col = sink_logits.reshape(kv_local, grouping)[None, :, :, None]
    top = jnp.maximum(jnp.max(scores, axis=-1), sink_col)
    expo = jnp.exp(scores - top[..., None])
    total = jnp.sum(expo, axis=-1) + jnp.exp(sink_col - top)
    probs = (expo / total[..., None]).astype(jnp.bfloat16)
    result = jnp.einsum(
        "nhgqk,nkhd->nqhgd", probs, value_blocks, preferred_element_type=jnp.float32
    )
    return result.astype(jnp.bfloat16).reshape(length, queries.shape[1])


def causal_local(upward, earlier, kernel):
    length = upward.shape[0]
    padded = jnp.concatenate([earlier, upward], axis=0).astype(jnp.float32)
    result = jnp.zeros(upward.shape, jnp.float32)
    for tap_index in range(kernel.shape[0]):
        result = result + kernel[tap_index][None, :] * padded[tap_index : tap_index + length]
    return result


def on_device_plain(
    queries,
    key_states,
    value_states,
    sink_logits,
    out_weight,
    residual,
    gain_attn,
    gain_before,
    gain_after,
    gate_weight,
    value_weight,
    gate_taps,
    value_taps,
    down_weight,
):
    length = queries.shape[0]
    attended = attention_local(queries, key_states, value_states, sink_logits)
    selected = attended
    attn_proj = lax.psum_scatter(
        jnp.dot(selected, out_weight, preferred_element_type=jnp.float32).astype(jnp.bfloat16),
        "tp",
        scatter_dimension=0,
        tiled=True,
    ).astype(jnp.float32)
    middle = residual.astype(jnp.float32) + rms_scale(attn_proj) * gain_attn
    normed = (rms_scale(middle) * gain_before).astype(jnp.bfloat16)
    whole_rows = lax.all_gather(normed, "tp", axis=0, tiled=True)
    gate_full, value_full = (
        lax.all_gather(gate_weight, "sp", axis=0, tiled=True),
        lax.all_gather(value_weight, "sp", axis=0, tiled=True),
    )
    gate_up = jnp.dot(whole_rows, gate_full, preferred_element_type=jnp.float32).astype(
        jnp.bfloat16
    )
    value_up = jnp.dot(whole_rows, value_full, preferred_element_type=jnp.float32).astype(
        jnp.bfloat16
    )
    reach = gate_taps.shape[0] - 1
    gate_before, value_before = passed_along(
        (gate_up[length - reach :], value_up[length - reach :]), "sp", 1
    )
    gate_conv = causal_local(gate_up, gate_before, gate_taps)
    value_conv = causal_local(value_up, value_before, value_taps)
    hidden = (jax.nn.silu(gate_conv) * value_conv).astype(jnp.bfloat16)
    down_whole = lax.all_gather(down_weight, "sp", axis=1, tiled=True)
    selected = hidden
    down = lax.psum_scatter(
        jnp.dot(selected, down_whole, preferred_element_type=jnp.float32).astype(jnp.bfloat16),
        "tp",
        scatter_dimension=0,
        tiled=True,
    ).astype(jnp.float32)
    return (middle + rms_scale(down) * gain_after).astype(jnp.bfloat16)


def team_peer(place, turn):
    low, high = place % 2, place // 2
    if turn & 1:
        low = 1 - low
    if turn & 2:
        high = 1 - high
    return high * 2 + low


def remote(src, dst, send, recv, **device):
    return pltpu.make_async_remote_copy(
        src_ref=src, dst_ref=dst, send_sem=send, recv_sem=recv, device_id=device, device_id_type=MESH
    )


def row_scale(block):
    return lax.rsqrt(jnp.mean(block * block, axis=-1, keepdims=True) + 1e-06)


def rows_by_units(rows, weight):
    return lax.dot_general(
        rows, weight, (((1,), (1,)), ((), ())), preferred_element_type=jnp.float32
    )


def even_parts(total, wanted):
    for parts in range(wanted, 0, -1):
        if total % (parts * 16) == 0:
            return parts


def layer_kernel(
    ring,
    q_ref,
    k_ref,
    v_ref,
    sink_ref,
    ow_far,
    res_far,
    ga_ref,
    gb_ref,
    gc_ref,
    gate_far,
    value_far,
    down_far,
    gate_taps,
    value_taps,
    out_ref,
    ow,
    res,
    mid,
    gate_all,
    value_all,
    down_all,
    rows_all,
    gate_up,
    value_up,
    hid,
    taps,
    k_ext,
    v_ext,
    att,
    snd,
    rcv,
    own,
    psnd,
    prcv,
    mine,
    keep,
    h1s,
    h1r,
    h2s,
    h2r,
    total,
    halo_s,
    halo_r,
    trade_s,
    trade_r,
    local_sem,
    first_s,
    first_r,
    next_s,
    next_r,
    half_s,
    half_r,
    pair_s,
    pair_r,
    rows_s,
    rows_r,
    mate_s,
    mate_r,
    edge_s,
    edge_r,
    sum_s,
    sum_r,
):
    sp, tp = lax.axis_index("sp"), lax.axis_index("tp")
    members = ring * TEAM
    level, place = sp // TEAM, sp % TEAM
    mate = 1 - tp
    length = q_ref.shape[0]
    share = length // 2
    units = gate_all.shape[0]
    wide = gate_far.shape[1]
    last = ring - 2
    sends = []

    def peer(turn):
        return level * TEAM + team_peer(place, turn)

    has_up, has_down = level < ring - 1, level > 0
    has_after, has_before = sp < members - 1, sp > 0

    barrier = pltpu.get_barrier_semaphore()

    def greet(**device):
        pl.semaphore_signal(barrier, inc=1, device_id=device, device_id_type=MESH)

    greet(tp=mate)
    for turn in (1, 2, 3):
        greet(sp=peer(turn))
    pl.when(has_up)(lambda: greet(sp=sp + TEAM))
    pl.when(has_down)(lambda: greet(sp=sp - TEAM))
    pl.when(has_after)(lambda: greet(sp=sp + 1))
    pl.when(has_before)(lambda: greet(sp=sp - 1))
    others = sum(jnp.where(there, 1, 0) for there in (has_up, has_down, has_after, has_before))
    pl.semaphore_wait(barrier, TEAM + others)

    def begin(copy, there=None):
        if there is None:
            copy.start()
        else:
            pl.when(there)(copy.start)
        sends.append((there, copy))
        return copy

    def arrive(copy, there=None):
        if there is None:
            copy.wait_recv()
        else:
            pl.when(there)(copy.wait_recv)

    halos = [
        begin(
            remote(
                ref.at[pl.ds(length - WINDOW, WINDOW)],
                ext.at[pl.ds(0, WINDOW)],
                halo_s.at[i],
                halo_r.at[i],
                sp=sp + 1,
            ),
            has_after,
        )
        for i, (ref, ext) in enumerate(((k_ref, k_ext), (v_ref, v_ext)))
    ]

    fars = (gate_far, value_far, down_far)
    wholes = (gate_all, value_all, down_all)

    def span(m, start, size):
        return wholes[m].at[:, pl.ds(pl.multiple_of(start * wide, wide), size * wide)]

    def piece(m, member):
        return fars[m].at[pl.ds(pl.multiple_of(member * units, units), units)]

    def can_send(side, step):
        return has_up & (level >= step) if side == 0 else has_down & (level + step < ring)

    def can_receive(side, step):
        return level > step if side == 0 else level + step < ring - 1

    def toward(side):
        return sp + TEAM if side == 0 else sp - TEAM

    def first_copy(m, side, q, source=None):
        block = span(m, level * TEAM + q, 1)
        return remote(
            block if source is None else source,
            block,
            first_s.at[m, side, q],
            first_r.at[m, side, q],
            sp=toward(side),
        )

    def next_copy(m, side, step, block, half=None):
        if half is None:
            part = span(m, block * TEAM, TEAM)
            sems = next_s.at[m, side, step - 1], next_r.at[m, side, step - 1]
        else:
            part = span(m, block * TEAM + half * (TEAM // 2), TEAM // 2)
            sems = half_s.at[side, step - 1, half], half_r.at[side, step - 1, half]
        return remote(part, part, *sems, sp=toward(side))

    def came(side, step):
        return level - 1 - step if side == 0 else level + 1 + step

    def receive(m, step, half=None):
        for side in range(2):
            there = can_receive(side, step)
            if step == 0:
                members_in = range(TEAM) if half is None else range(half * 2, half * 2 + 2)
                for q in members_in:
                    block = span(m, came(side, 0) * TEAM + q, 1)
                    sems = first_s.at[m, side, q], first_r.at[m, side, q]
                    arrive(remote(block, block, *sems, sp=toward(side)), there)
            else:
                arrive(next_copy(m, side, step, came(side, step), half), there)

    def pass_on(m, step, half=None):
        receive(m, step - 1, half)
        for side in range(2):
            block = level - step if side == 0 else level + step
            begin(next_copy(m, side, step, block, half), can_send(side, step))

    trades, locals_ = [], []
    for m in range(3):
        trades.append(
            {
                turn: begin(
                    remote(
                        piece(m, team_peer(place, turn)),
                        span(m, sp, 1),
                        trade_s.at[m, turn - 1],
                        trade_r.at[m, turn - 1],
                        sp=peer(turn),
                    )
                )
                for turn in (3, 1, 2)
            }
        )
        for side in range(2):
            begin(first_copy(m, side, place, piece(m, place)), can_send(side, 0))
        copy = pltpu.make_async_copy(piece(m, place), span(m, sp, 1), local_sem.at[m])
        copy.start()
        locals_.append(copy)
    fetch_ow = pltpu.make_async_copy(ow_far, ow, local_sem.at[3])
    fetch_ow.start()
    fetch_res = pltpu.make_async_copy(res_far, res, local_sem.at[4])
    fetch_res.start()

    def first_rest(m):
        for turn in (1, 2, 3):
            trades[m][turn].wait_recv()
            for side in range(2):
                begin(first_copy(m, side, team_peer(place, turn)), can_send(side, 0))

    pending = [(m, step) for step in range(1, last + 1) for m in range(2)]

    def pass_next(count):
        for m, step in pending[:count]:
            pass_on(m, step)
        del pending[:count]

    k_ext[pl.ds(WINDOW, length)] = k_ref[...]
    v_ext[pl.ds(WINDOW, length)] = v_ref[...]

    @pl.when(jnp.logical_not(has_before))
    def _():
        k_ext[pl.ds(0, WINDOW)] = jnp.zeros((WINDOW, k_ref.shape[1]), k_ref.dtype)
        v_ext[pl.ds(0, WINDOW)] = jnp.zeros((WINDOW, k_ref.shape[1]), k_ref.dtype)

    for p in range(TEAM):

        @pl.when(place == p)
        def _(p=p):
            for i, ref in enumerate((gate_taps, value_taps)):
                taps[i, : ref.shape[0]] = ref[:, p * units : (p + 1) * units]

    for copy in halos:
        arrive(copy, has_before)
    heads_kv = k_ref.shape[1] // HD
    grouping = q_ref.shape[1] // k_ref.shape[1]
    row = lax.broadcasted_iota(jnp.int32, (WINDOW, 2 * WINDOW), 0)
    col = lax.broadcasted_iota(jnp.int32, (WINDOW, 2 * WINDOW), 1)
    band = (col <= row + WINDOW) & (col > row)

    for kv in range(heads_kv):

        def block_step(n, carry, kv=kv):
            start = pl.multiple_of(n * WINDOW, WINDOW)
            keys = k_ext[pl.ds(start, 2 * WINDOW), kv * HD : (kv + 1) * HD]
            values = v_ext[pl.ds(start, 2 * WINDOW), kv * HD : (kv + 1) * HD]
            wide_q = q_ref[pl.ds(start, WINDOW), kv * grouping * HD : (kv + 1) * grouping * HD]
            visible = band & (col + (sp * length + start - WINDOW) >= 0)
            stacked = jnp.concatenate(
                [wide_q[:, g * HD : (g + 1) * HD] for g in range(grouping)], axis=0
            )
            scores = lax.dot_general(
                stacked, keys, (((1,), (1,)), ((), ())), preferred_element_type=jnp.float32
            ) * HD ** (-0.5)
            probs = []
            for g in range(grouping):
                sink = sink_ref[kv * grouping + g]
                part = jnp.where(visible, scores[g * WINDOW : (g + 1) * WINDOW], NEG_FILL)
                top = jnp.maximum(jnp.max(part, axis=-1, keepdims=True), sink)
                expo = jnp.exp(part - top)
                whole = jnp.sum(expo, axis=-1, keepdims=True) + jnp.exp(sink - top)
                probs.append((expo / whole).astype(jnp.bfloat16))
            result = jnp.dot(
                jnp.concatenate(probs, axis=0), values, preferred_element_type=jnp.float32
            ).astype(jnp.bfloat16)
            att[pl.ds(start, WINDOW), kv * grouping * HD : (kv + 1) * grouping * HD] = (
                jnp.concatenate(
                    [result[g * WINDOW : (g + 1) * WINDOW] for g in range(grouping)], axis=1
                )
            )
            return carry

        lax.fori_loop(0, length // WINDOW, block_step, 0)
    first_rest(0)

    columns = ow.shape[1]
    tile = min(512, columns)
    fetch_ow.wait()

    def project(rows_start, target):
        def tile_step(t, carry):
            at = pl.multiple_of(t * tile, tile)
            target[:, pl.ds(at, tile)] = jnp.dot(
                att[pl.ds(rows_start, share)],
                ow[:, pl.ds(at, tile)],
                preferred_element_type=jnp.float32,
            ).astype(jnp.bfloat16)
            return carry

        lax.fori_loop(0, columns // tile, tile_step, 0)

    project(pl.multiple_of(mate * share, share), snd)
    pair = begin(remote(snd, rcv, pair_s, pair_r, tp=mate))
    project(pl.multiple_of(tp * share, share), own)
    first_rest(1)
    fetch_res.wait()
    pair.wait_recv()
    band_rows = 32
    rows = length * TEAM
    edge = rows_all.shape[0] - rows

    def row_start(member, core):
        return pl.multiple_of(edge + (member * 2 + core) * share, edge)

    my_rows = row_start(place, tp)

    def norm_step(t, carry):
        at = pl.ds(pl.multiple_of(t * band_rows, band_rows), band_rows)
        proj = own[at].astype(jnp.float32) + rcv[at].astype(jnp.float32)
        middle = res[at].astype(jnp.float32) + proj * row_scale(proj) * ga_ref[...]
        mid[at] = middle
        rows_all[pl.ds(pl.multiple_of(my_rows + t * band_rows, edge), band_rows)] = (
            middle * row_scale(middle) * gb_ref[...]
        ).astype(jnp.bfloat16)
        return carry

    lax.fori_loop(0, share // band_rows, norm_step, 0)

    def slot(member, first=0, size=share):
        start = pl.multiple_of(row_start(member, tp) + first, edge)
        return rows_all.at[pl.ds(start, size)]

    def row_copy(block, i, turn):
        return begin(remote(block, block, rows_s.at[i], rows_r.at[i], sp=peer(turn)))

    def to_mate(block, i):
        return begin(remote(block, block, mate_s.at[i], mate_r.at[i], tp=mate))

    half = share // 2
    mine_rows = slot(place)
    across = [row_copy(mine_rows, 0, 1), row_copy(mine_rows, 1, 2)]
    mates = [to_mate(mine_rows, 0)]
    pass_next(2)
    across[0].wait_recv()
    across.append(row_copy(slot(team_peer(place, 1), 0, half), 2, 2))
    mates.append(to_mate(slot(team_peer(place, 1)), 1))
    across[1].wait_recv()
    across.append(row_copy(slot(team_peer(place, 2), half, half), 3, 1))
    mates.append(to_mate(slot(team_peer(place, 2)), 2))
    pass_next(1)
    across[2].wait_recv()
    across[3].wait_recv()
    mates.append(to_mate(slot(team_peer(place, 3)), 3))
    for copy in mates:
        copy.wait_recv()
    ending = remote(
        rows_all.at[pl.ds(rows, edge)], rows_all.at[pl.ds(0, edge)], edge_s, edge_r, sp=sp + TEAM
    )
    begin(ending, has_up)

    @pl.when(jnp.logical_not(has_down))
    def _():
        rows_all[pl.ds(0, edge)] = jnp.zeros((edge, rows_all.shape[1]), rows_all.dtype)

    pass_next(len(pending))
    arrive(ending, has_down)

    steps = even_parts(rows + edge, 4)
    chunk = (rows + edge) // steps

    def up(m, result):
        receive(m, last)
        locals_[m].wait()

        def up_step(t, carry):
            at = pl.ds(pl.multiple_of(t * chunk, edge), chunk)
            result[at] = rows_by_units(rows_all[at], wholes[m][...]).astype(jnp.bfloat16)
            return carry

        lax.fori_loop(0, steps, up_step, 0)

    up(0, gate_up)
    first_rest(2)
    up(1, value_up)
    reach = gate_taps.shape[0] - 1
    conv_rows = 64
    per = share // conv_rows

    def conv_step(t, carry):
        at = pl.multiple_of(t * conv_rows, conv_rows)

        def mixed(source, i):
            padded = source[pl.ds(at, conv_rows + edge)].astype(jnp.float32)
            result = jnp.zeros((conv_rows, units), jnp.float32)
            for k in range(reach + 1):
                first = edge - reach + k
                result = result + taps[i, k : k + 1, :] * padded[first : first + conv_rows]
            return result

        gate = mixed(gate_up, 0)
        value = mixed(value_up, 1)
        group = t // per
        to = (group % 2 * TEAM + group // 2) * share + t % per * conv_rows
        hid[pl.ds(pl.multiple_of(to, conv_rows), conv_rows)] = (
            gate / (1.0 + jnp.exp(-gate)) * value
        ).astype(jnp.bfloat16)
        return carry

    lax.fori_loop(0, rows // conv_rows, conv_step, 0)

    locals_[2].wait()
    pairs = jnp.minimum(level, ring - 1 - level)

    def block_at(i):
        near = jnp.where(i % 2 == 1, level - (i + 1) // 2, level + i // 2)
        return jnp.where(i <= 2 * pairs, near, jnp.where(level < ring // 2, i, ring - 1 - i))

    group_cols = TEAM // 2 * wide
    jobs = [(i, h) for i in range(ring) for h in range(2)]

    def cols_of(j):
        i, h = jobs[j]
        return pl.ds(
            pl.multiple_of((block_at(i) * TEAM + h * (TEAM // 2)) * wide, group_cols), group_cols
        )

    def turns_of(j):
        return (1, 2) if j % 2 == 0 else (2, 1)

    many = TEAM * share
    half_many = many // 2

    def product(core, cols, store):
        def step(t, carry):
            at = pl.multiple_of(t * half_many, half_many)
            store(
                pl.ds(at, half_many),
                jnp.dot(
                    hid[pl.ds(pl.multiple_of(core * many + at, half_many), half_many)],
                    down_all[:, cols],
                    preferred_element_type=jnp.float32,
                ).astype(jnp.bfloat16),
            )
            return carry

        lax.fori_loop(0, 2, step, 0)

    twos, ones, seconds = {}, {}, {}

    def stage_product(j):
        i, h = jobs[j]
        if i >= 1:
            if i <= last:
                pass_on(2, i, h)
            else:
                receive(2, last, h)
        cols = cols_of(j)

        def away(at, part):
            psnd[j, at] = part

        def here(at, part):
            mine[j % 2, at] = part

        product(mate, cols, away)
        twos[j] = begin(remote(psnd.at[j], prcv.at[j], sum_s.at[0, j], sum_r.at[0, j], tp=mate))
        product(tp, cols, here)

    def shard(j, turn):
        at = pl.ds(pl.multiple_of(team_peer(place, turn) * share, share), share)
        return mine[j % 2, at].astype(jnp.float32) + prcv[j, at].astype(jnp.float32)

    def stage_first(j):
        one, two = turns_of(j)
        twos[j].wait_recv()
        h1s[j, 0] = shard(j, one).astype(jnp.bfloat16)
        h1s[j, 1] = shard(j, 3).astype(jnp.bfloat16)
        ones[j] = begin(
            remote(h1s.at[j], h1r.at[j], sum_s.at[1, j], sum_r.at[1, j], sp=peer(one))
        )
        total[:, cols_of(j)] = shard(j, 0)
        keep[j % 2] = shard(j, two)

    def stage_second(j):
        one, two = turns_of(j)
        ones[j].wait_recv()
        h2s[j] = (keep[j % 2] + h1r[j, 1].astype(jnp.float32)).astype(jnp.bfloat16)
        seconds[j] = begin(
            remote(h2s.at[j], h2r.at[j], sum_s.at[2, j], sum_r.at[2, j], sp=peer(two))
        )
        total[:, cols_of(j)] += h1r[j, 0].astype(jnp.float32)

    def stage_last(j):
        seconds[j].wait_recv()
        total[:, cols_of(j)] += h2r[j].astype(jnp.float32)

    stages = (stage_product, stage_first, stage_second, stage_last)
    for clock in range(len(jobs) + len(stages) - 1):
        for late in reversed(range(len(stages))):
            if 0 <= clock - late < len(jobs):
                stages[late](clock - late)

    def out_step(t, carry):
        at = pl.ds(pl.multiple_of(t * band_rows, band_rows), band_rows)
        block = total[at]
        out_ref[at] = (mid[at] + block * row_scale(block) * gc_ref[...]).astype(out_ref.dtype)
        return carry

    lax.fori_loop(0, share // band_rows, out_step, 0)
    for there, copy in sends:
        if there is None:
            copy.wait_send()
        else:
            pl.when(there)(copy.wait_send)


def on_device_team(
    ring,
    queries,
    key_states,
    value_states,
    sink_logits,
    out_weight,
    residual,
    gain_attn,
    gain_before,
    gain_after,
    gate_weight,
    value_weight,
    gate_taps,
    value_taps,
    down_weight,
):
    length, width = queries.shape[0], residual.shape[1]
    share = residual.shape[0]
    wide, local_units = gate_weight.shape
    units = local_units // TEAM
    rows = length * TEAM
    edge = 16
    vmem = pl.BlockSpec(memory_space=pltpu.VMEM)
    smem = pl.BlockSpec(memory_space=pltpu.SMEM)
    far = pl.BlockSpec(memory_space=pl.ANY)
    dma = pltpu.SemaphoreType.DMA
    bf16, f32 = jnp.bfloat16, jnp.float32
    jobs, group_cols = ring * 2, TEAM // 2 * wide

    def buffer(*shape, dtype=bf16):
        return pltpu.VMEM(shape, dtype)

    return pl.pallas_call(
        functools.partial(layer_kernel, ring),
        out_shape=jax.ShapeDtypeStruct((share, width), bf16),
        in_specs=[vmem] * 3 + [smem] + [far] * 2 + [vmem] * 3 + [far] * 3 + [vmem] * 2,
        out_specs=vmem,
        scratch_shapes=[
            buffer(*out_weight.shape),
            buffer(share, width),
            buffer(share, width, dtype=f32),
            buffer(units, width),
            buffer(units, width),
            buffer(units, width),
            buffer(rows + edge, width),
            buffer(rows + edge, units),
            buffer(rows + edge, units),
            buffer(rows, units),
            buffer(2, 8, units, dtype=f32),
            buffer(length + WINDOW, key_states.shape[1]),
            buffer(length + WINDOW, key_states.shape[1]),
            buffer(*queries.shape),
            buffer(share, width),
            buffer(share, width),
            buffer(share, width),
            buffer(jobs, TEAM * share, group_cols),
            buffer(jobs, TEAM * share, group_cols),
            buffer(2, TEAM * share, group_cols),
            buffer(2, share, group_cols, dtype=f32),
            buffer(jobs, 2, share, group_cols),
            buffer(jobs, 2, share, group_cols),
            buffer(jobs, share, group_cols),
            buffer(jobs, share, group_cols),
            buffer(share, width, dtype=f32),
            dma((2,)),
            dma((2,)),
            dma((3, TEAM - 1)),
            dma((3, TEAM - 1)),
            dma((5,)),
            dma((3, 2, TEAM)),
            dma((3, 2, TEAM)),
            dma((2, 2, ring - 2)),
            dma((2, 2, ring - 2)),
            dma((2, ring - 2, 2)),
            dma((2, ring - 2, 2)),
            dma(()),
            dma(()),
            dma((4,)),
            dma((4,)),
            dma((TEAM,)),
            dma((TEAM,)),
            dma(()),
            dma(()),
            dma((3, jobs)),
            dma((3, jobs)),
        ],
        compiler_params=pltpu.CompilerParams(
            collective_id=0, has_side_effects=True, vmem_limit_bytes=VMEM_BYTES
        ),
        name="layer",
    )(
        queries,
        key_states,
        value_states,
        sink_logits,
        out_weight,
        residual,
        gain_attn[None],
        gain_before[None],
        gain_after[None],
        gate_weight.T,
        value_weight.T,
        down_weight,
        gate_taps,
        value_taps,
    )


def solution(mesh):
    in_specs = (
        P("sp", "tp"),
        P("sp", "tp"),
        P("sp", "tp"),
        P("tp"),
        P("tp", None),
        P(("sp", "tp"), None),
        P(),
        P(),
        P(),
        P("sp", "tp"),
        P("sp", "tp"),
        P(None, "tp"),
        P(None, "tp"),
        P("tp", "sp"),
    )
    out_specs = P(("sp", "tp"), None)
    members, cores = mesh.shape["sp"], mesh.shape["tp"]
    ring = members // TEAM

    def on_device(*args):
        units, wide = args[13].shape
        teams = cores == 2 and members % TEAM == 0 and ring >= 3
        if teams and units % (TEAM * 16) == 0 and wide % 128 == 0:
            return on_device_team(ring, *args)
        return on_device_plain(*args)

    return jax.shard_map(
        on_device, mesh=mesh, in_specs=in_specs, out_specs=out_specs, check_vma=False
    )
```

```python
import functools

import jax
import jax.numpy as jnp
from jax import lax
from jax.experimental import pallas as pl
from jax.experimental.pallas import tpu as pltpu
from jax.sharding import PartitionSpec as P

HD = 64
WINDOW = 128
TEAM = 4


NEG_FILL = -1e30
MESH = pl.DeviceIdType.MESH
VMEM_BYTES = 63 * 1024 * 1024

def passed_along(block, axis, distance):
    devices = range(lax.axis_size(axis))
    route = [(i - distance, i) for i in devices if i - distance in devices]
    return lax.ppermute(block, axis, route)


def rms_scale(matrix):
    return matrix * lax.rsqrt(jnp.mean(matrix * matrix, axis=-1, keepdims=True) + 1e-06)


def attention_local(queries, key_states, value_states, sink_logits):
    length = queries.shape[0]
    blocks = length // WINDOW
    kv_local = key_states.shape[1] // HD
    grouping = queries.shape[1] // key_states.shape[1]
    earlier_keys, earlier_values = passed_along(
        (key_states[length - WINDOW :], value_states[length - WINDOW :]), "sp", 1
    )
    keys_ext = jnp.concatenate([earlier_keys, key_states], axis=0).reshape(
        blocks + 1, WINDOW, kv_local, HD
    )
    values_ext = jnp.concatenate([earlier_values, value_states], axis=0).reshape(
        blocks + 1, WINDOW, kv_local, HD
    )
    key_blocks = jnp.concatenate([keys_ext[:-1], keys_ext[1:]], axis=1)
    value_blocks = jnp.concatenate([values_ext[:-1], values_ext[1:]], axis=1)
    query_blocks = queries.reshape(blocks, WINDOW, kv_local, grouping, HD)
    offset = lax.axis_index("sp") * length
    qpos = (offset + jnp.arange(length, dtype=jnp.int32)).reshape(blocks, WINDOW)
    kpos = jnp.concatenate([qpos - WINDOW, qpos], axis=1)
    visible = (
        (kpos[:, None, :] <= qpos[:, :, None])
        & (qpos[:, :, None] - kpos[:, None, :] < WINDOW)
        & (kpos[:, None, :] >= 0)
    )
    scores = jnp.einsum(
        "nqhgd,nkhd->nhgqk", query_blocks, key_blocks, preferred_element_type=jnp.float32
    ) * HD ** (-0.5)
    scores = jnp.where(visible[:, None, None], scores, NEG_FILL)
    sink_col = sink_logits.reshape(kv_local, grouping)[None, :, :, None]
    top = jnp.maximum(jnp.max(scores, axis=-1), sink_col)
    expo = jnp.exp(scores - top[..., None])
    total = jnp.sum(expo, axis=-1) + jnp.exp(sink_col - top)
    probs = (expo / total[..., None]).astype(jnp.bfloat16)
    result = jnp.einsum(
        "nhgqk,nkhd->nqhgd", probs, value_blocks, preferred_element_type=jnp.float32
    )
    return result.astype(jnp.bfloat16).reshape(length, queries.shape[1])


def causal_local(upward, earlier, kernel):
    length = upward.shape[0]
    padded = jnp.concatenate([earlier, upward], axis=0).astype(jnp.float32)
    result = jnp.zeros(upward.shape, jnp.float32)
    for tap_index in range(kernel.shape[0]):
        result = result + kernel[tap_index][None, :] * padded[tap_index : tap_index + length]
    return result


def on_device_plain(
    queries,
    key_states,
    value_states,
    sink_logits,
    out_weight,
    residual,
    gain_attn,
    gain_before,
    gain_after,
    gate_weight,
    value_weight,
    gate_taps,
    value_taps,
    down_weight,
):
    length = queries.shape[0]
    attended = attention_local(queries, key_states, value_states, sink_logits)
    selected = attended
    attn_proj = lax.psum_scatter(
        jnp.dot(selected, out_weight, preferred_element_type=jnp.float32).astype(jnp.bfloat16),
        "tp",
        scatter_dimension=0,
        tiled=True,
    ).astype(jnp.float32)
    middle = residual.astype(jnp.float32) + rms_scale(attn_proj) * gain_attn
    normed = (rms_scale(middle) * gain_before).astype(jnp.bfloat16)
    whole_rows = lax.all_gather(normed, "tp", axis=0, tiled=True)
    gate_full, value_full = (
        lax.all_gather(gate_weight, "sp", axis=0, tiled=True),
        lax.all_gather(value_weight, "sp", axis=0, tiled=True),
    )
    gate_up = jnp.dot(whole_rows, gate_full, preferred_element_type=jnp.float32).astype(
        jnp.bfloat16
    )
    value_up = jnp.dot(whole_rows, value_full, preferred_element_type=jnp.float32).astype(
        jnp.bfloat16
    )
    reach = gate_taps.shape[0] - 1
    gate_before, value_before = passed_along(
        (gate_up[length - reach :], value_up[length - reach :]), "sp", 1
    )
    gate_conv = causal_local(gate_up, gate_before, gate_taps)
    value_conv = causal_local(value_up, value_before, value_taps)
    hidden = (jax.nn.silu(gate_conv) * value_conv).astype(jnp.bfloat16)
    down_whole = lax.all_gather(down_weight, "sp", axis=1, tiled=True)
    selected = hidden
    down = lax.psum_scatter(
        jnp.dot(selected, down_whole, preferred_element_type=jnp.float32).astype(jnp.bfloat16),
        "tp",
        scatter_dimension=0,
        tiled=True,
    ).astype(jnp.float32)
    return (middle + rms_scale(down) * gain_after).astype(jnp.bfloat16)


def team_peer(place, turn):
    low, high = place % 2, place // 2
    if turn & 1:
        low = 1 - low
    if turn & 2:
        high = 1 - high
    return high * 2 + low


def remote(src, dst, send, recv, **device):
    return pltpu.make_async_remote_copy(
        src_ref=src, dst_ref=dst, send_sem=send, recv_sem=recv, device_id=device, device_id_type=MESH
    )


def row_scale(block):
    return lax.rsqrt(jnp.mean(block * block, axis=-1, keepdims=True) + 1e-06)


def rows_by_units(rows, weight):
    return lax.dot_general(
        rows, weight, (((1,), (1,)), ((), ())), preferred_element_type=jnp.float32
    )


def even_parts(total, wanted):
    for parts in range(wanted, 0, -1):
        if total % (parts * 16) == 0:
            return parts


def layer_kernel(
    ring,
    q_ref,
    k_ref,
    v_ref,
    sink_ref,
    ow_far,
    res_far,
    ga_ref,
    gb_ref,
    gc_ref,
    gate_far,
    value_far,
    down_far,
    gate_taps,
    value_taps,
    out_ref,
    ow,
    res,
    mid,
    gate_all,
    value_all,
    down_all,
    rows_all,
    gate_up,
    value_up,
    hid,
    taps,
    k_ext,
    v_ext,
    att,
    snd,
    rcv,
    own,
    psnd,
    prcv,
    mine,
    keep,
    h1s,
    h1r,
    h2s,
    h2r,
    total,
    halo_s,
    halo_r,
    trade_s,
    trade_r,
    local_sem,
    first_s,
    first_r,
    next_s,
    next_r,
    half_s,
    half_r,
    pair_s,
    pair_r,
    rows_s,
    rows_r,
    mate_s,
    mate_r,
    edge_s,
    edge_r,
    sum_s,
    sum_r,
):
    sp, tp = lax.axis_index("sp"), lax.axis_index("tp")
    members = ring * TEAM
    level, place = sp // TEAM, sp % TEAM
    mate = 1 - tp
    length = q_ref.shape[0]
    share = length // 2
    units = gate_all.shape[0]
    wide = gate_far.shape[1]
    last = ring - 2
    sends = []

    def peer(turn):
        return level * TEAM + team_peer(place, turn)

    has_up, has_down = level < ring - 1, level > 0
    has_after, has_before = sp < members - 1, sp > 0

    barrier = pltpu.get_barrier_semaphore()

    def greet(**device):
        pl.semaphore_signal(barrier, inc=1, device_id=device, device_id_type=MESH)

    greet(tp=mate)
    for turn in (1, 2, 3):
        greet(sp=peer(turn))
    pl.when(has_up)(lambda: greet(sp=sp + TEAM))
    pl.when(has_down)(lambda: greet(sp=sp - TEAM))
    pl.when(has_after)(lambda: greet(sp=sp + 1))
    pl.when(has_before)(lambda: greet(sp=sp - 1))
    others = sum(jnp.where(there, 1, 0) for there in (has_up, has_down, has_after, has_before))
    pl.semaphore_wait(barrier, TEAM + others)

    def begin(copy, there=None):
        if there is None:
            copy.start()
        else:
            pl.when(there)(copy.start)
        sends.append((there, copy))
        return copy

    def arrive(copy, there=None):
        if there is None:
            copy.wait_recv()
        else:
            pl.when(there)(copy.wait_recv)

    halos = [
        begin(
            remote(
                ref.at[pl.ds(length - WINDOW, WINDOW)],
                ext.at[pl.ds(0, WINDOW)],
                halo_s.at[i],
                halo_r.at[i],
                sp=sp + 1,
            ),
            has_after,
        )
        for i, (ref, ext) in enumerate(((k_ref, k_ext), (v_ref, v_ext)))
    ]

    fars = (gate_far, value_far, down_far)
    wholes = (gate_all, value_all, down_all)

    def span(m, start, size):
        return wholes[m].at[:, pl.ds(pl.multiple_of(start * wide, wide), size * wide)]

    def piece(m, member):
        return fars[m].at[pl.ds(pl.multiple_of(member * units, units), units)]

    def can_send(side, step):
        return has_up & (level >= step) if side == 0 else has_down & (level + step < ring)

    def can_receive(side, step):
        return level > step if side == 0 else level + step < ring - 1

    def toward(side):
        return sp + TEAM if side == 0 else sp - TEAM

    def first_copy(m, side, q, source=None):
        block = span(m, level * TEAM + q, 1)
        return remote(
            block if source is None else source,
            block,
            first_s.at[m, side, q],
            first_r.at[m, side, q],
            sp=toward(side),
        )

    def next_copy(m, side, step, block, half=None):
        if half is None:
            part = span(m, block * TEAM, TEAM)
            sems = next_s.at[m, side, step - 1], next_r.at[m, side, step - 1]
        else:
            part = span(m, block * TEAM + half * (TEAM // 2), TEAM // 2)
            sems = half_s.at[side, step - 1, half], half_r.at[side, step - 1, half]
        return remote(part, part, *sems, sp=toward(side))

    def came(side, step):
        return level - 1 - step if side == 0 else level + 1 + step

    def receive(m, step, half=None):
        for side in range(2):
            there = can_receive(side, step)
            if step == 0:
                members_in = range(TEAM) if half is None else range(half * 2, half * 2 + 2)
                for q in members_in:
                    block = span(m, came(side, 0) * TEAM + q, 1)
                    sems = first_s.at[m, side, q], first_r.at[m, side, q]
                    arrive(remote(block, block, *sems, sp=toward(side)), there)
            else:
                arrive(next_copy(m, side, step, came(side, step), half), there)

    def pass_on(m, step, half=None):
        receive(m, step - 1, half)
        for side in range(2):
            block = level - step if side == 0 else level + step
            begin(next_copy(m, side, step, block, half), can_send(side, step))

    trades, locals_ = [], []
    for m in range(3):
        trades.append(
            {
                turn: begin(
                    remote(
                        piece(m, team_peer(place, turn)),
                        span(m, sp, 1),
                        trade_s.at[m, turn - 1],
                        trade_r.at[m, turn - 1],
                        sp=peer(turn),
                    )
                )
                for turn in (3, 1, 2)
            }
        )
        for side in range(2):
            begin(first_copy(m, side, place, piece(m, place)), can_send(side, 0))
        copy = pltpu.make_async_copy(piece(m, place), span(m, sp, 1), local_sem.at[m])
        copy.start()
        locals_.append(copy)
    fetch_ow = pltpu.make_async_copy(ow_far, ow, local_sem.at[3])
    fetch_ow.start()
    fetch_res = pltpu.make_async_copy(res_far, res, local_sem.at[4])
    fetch_res.start()

    def first_rest(m):
        for turn in (1, 2, 3):
            trades[m][turn].wait_recv()
            for side in range(2):
                begin(first_copy(m, side, team_peer(place, turn)), can_send(side, 0))

    pending = [(m, step) for step in range(1, last + 1) for m in range(2)]

    def pass_next(count):
        for m, step in pending[:count]:
            pass_on(m, step)
        del pending[:count]

    k_ext[pl.ds(WINDOW, length)] = k_ref[...]
    v_ext[pl.ds(WINDOW, length)] = v_ref[...]

    @pl.when(jnp.logical_not(has_before))
    def _():
        k_ext[pl.ds(0, WINDOW)] = jnp.zeros((WINDOW, k_ref.shape[1]), k_ref.dtype)
        v_ext[pl.ds(0, WINDOW)] = jnp.zeros((WINDOW, k_ref.shape[1]), k_ref.dtype)

    for p in range(TEAM):

        @pl.when(place == p)
        def _(p=p):
            for i, ref in enumerate((gate_taps, value_taps)):
                taps[i, : ref.shape[0]] = ref[:, p * units : (p + 1) * units]

    for copy in halos:
        arrive(copy, has_before)
    heads_kv = k_ref.shape[1] // HD
    grouping = q_ref.shape[1] // k_ref.shape[1]
    row = lax.broadcasted_iota(jnp.int32, (WINDOW, 2 * WINDOW), 0)
    col = lax.broadcasted_iota(jnp.int32, (WINDOW, 2 * WINDOW), 1)
    band = (col <= row + WINDOW) & (col > row)

    for kv in range(heads_kv):

        def block_step(n, carry, kv=kv):
            start = pl.multiple_of(n * WINDOW, WINDOW)
            keys = k_ext[pl.ds(start, 2 * WINDOW), kv * HD : (kv + 1) * HD]
            values = v_ext[pl.ds(start, 2 * WINDOW), kv * HD : (kv + 1) * HD]
            wide_q = q_ref[pl.ds(start, WINDOW), kv * grouping * HD : (kv + 1) * grouping * HD]
            visible = band & (col + (sp * length + start - WINDOW) >= 0)
            stacked = jnp.concatenate(
                [wide_q[:, g * HD : (g + 1) * HD] for g in range(grouping)], axis=0
            )
            scores = lax.dot_general(
                stacked, keys, (((1,), (1,)), ((), ())), preferred_element_type=jnp.float32
            ) * HD ** (-0.5)
            probs = []
            for g in range(grouping):
                sink = sink_ref[kv * grouping + g]
                part = jnp.where(visible, scores[g * WINDOW : (g + 1) * WINDOW], NEG_FILL)
                top = jnp.maximum(jnp.max(part, axis=-1, keepdims=True), sink)
                expo = jnp.exp(part - top)
                whole = jnp.sum(expo, axis=-1, keepdims=True) + jnp.exp(sink - top)
                probs.append((expo / whole).astype(jnp.bfloat16))
            result = jnp.dot(
                jnp.concatenate(probs, axis=0), values, preferred_element_type=jnp.float32
            ).astype(jnp.bfloat16)
            att[pl.ds(start, WINDOW), kv * grouping * HD : (kv + 1) * grouping * HD] = (
                jnp.concatenate(
                    [result[g * WINDOW : (g + 1) * WINDOW] for g in range(grouping)], axis=1
                )
            )
            return carry

        lax.fori_loop(0, length // WINDOW, block_step, 0)
    first_rest(0)

    columns = ow.shape[1]
    tile = min(512, columns)
    fetch_ow.wait()

    def project(rows_start, target):
        def tile_step(t, carry):
            at = pl.multiple_of(t * tile, tile)
            target[:, pl.ds(at, tile)] = jnp.dot(
                att[pl.ds(rows_start, share)],
                ow[:, pl.ds(at, tile)],
                preferred_element_type=jnp.float32,
            ).astype(jnp.bfloat16)
            return carry

        lax.fori_loop(0, columns // tile, tile_step, 0)

    project(pl.multiple_of(mate * share, share), snd)
    pair = begin(remote(snd, rcv, pair_s, pair_r, tp=mate))
    project(pl.multiple_of(tp * share, share), own)
    first_rest(1)
    fetch_res.wait()
    pair.wait_recv()
    band_rows = 32
    rows = length * TEAM
    edge = rows_all.shape[0] - rows

    def row_start(member, core):
        return pl.multiple_of(edge + (member * 2 + core) * share, edge)

    my_rows = row_start(place, tp)

    def norm_step(t, carry):
        at = pl.ds(pl.multiple_of(t * band_rows, band_rows), band_rows)
        proj = own[at].astype(jnp.float32) + rcv[at].astype(jnp.float32)
        middle = res[at].astype(jnp.float32) + proj * row_scale(proj) * ga_ref[...]
        mid[at] = middle
        rows_all[pl.ds(pl.multiple_of(my_rows + t * band_rows, edge), band_rows)] = (
            middle * row_scale(middle) * gb_ref[...]
        ).astype(jnp.bfloat16)
        return carry

    lax.fori_loop(0, share // band_rows, norm_step, 0)

    def slot(member, first=0, size=share):
        start = pl.multiple_of(row_start(member, tp) + first, edge)
        return rows_all.at[pl.ds(start, size)]

    def row_copy(block, i, turn):
        return begin(remote(block, block, rows_s.at[i], rows_r.at[i], sp=peer(turn)))

    def to_mate(block, i):
        return begin(remote(block, block, mate_s.at[i], mate_r.at[i], tp=mate))

    half = share // 2
    mine_rows = slot(place)
    across = [row_copy(mine_rows, 0, 1), row_copy(mine_rows, 1, 2)]
    mates = [to_mate(mine_rows, 0)]
    pass_next(2)
    across[0].wait_recv()
    across.append(row_copy(slot(team_peer(place, 1), 0, half), 2, 2))
    mates.append(to_mate(slot(team_peer(place, 1)), 1))
    across[1].wait_recv()
    across.append(row_copy(slot(team_peer(place, 2), half, half), 3, 1))
    mates.append(to_mate(slot(team_peer(place, 2)), 2))
    pass_next(1)
    across[2].wait_recv()
    across[3].wait_recv()
    mates.append(to_mate(slot(team_peer(place, 3)), 3))
    for copy in mates:
        copy.wait_recv()
    ending = remote(
        rows_all.at[pl.ds(rows, edge)], rows_all.at[pl.ds(0, edge)], edge_s, edge_r, sp=sp + TEAM
    )
    begin(ending, has_up)

    @pl.when(jnp.logical_not(has_down))
    def _():
        rows_all[pl.ds(0, edge)] = jnp.zeros((edge, rows_all.shape[1]), rows_all.dtype)

    pass_next(len(pending))
    arrive(ending, has_down)

    steps = even_parts(rows + edge, 4)
    chunk = (rows + edge) // steps

    def up(m, result):
        receive(m, last)
        locals_[m].wait()

        def up_step(t, carry):
            at = pl.ds(pl.multiple_of(t * chunk, edge), chunk)
            result[at] = rows_by_units(rows_all[at], wholes[m][...]).astype(jnp.bfloat16)
            return carry

        lax.fori_loop(0, steps, up_step, 0)

    up(0, gate_up)
    first_rest(2)
    up(1, value_up)
    reach = gate_taps.shape[0] - 1
    conv_rows = 64
    per = share // conv_rows

    def conv_step(t, carry):
        at = pl.multiple_of(t * conv_rows, conv_rows)

        def mixed(source, i):
            padded = source[pl.ds(at, conv_rows + edge)].astype(jnp.float32)
            result = jnp.zeros((conv_rows, units), jnp.float32)
            for k in range(reach + 1):
                first = edge - reach + k
                result = result + taps[i, k : k + 1, :] * padded[first : first + conv_rows]
            return result

        gate = mixed(gate_up, 0)
        value = mixed(value_up, 1)
        group = t // per
        to = (group % 2 * TEAM + group // 2) * share + t % per * conv_rows
        hid[pl.ds(pl.multiple_of(to, conv_rows), conv_rows)] = (
            gate / (1.0 + jnp.exp(-gate)) * value
        ).astype(jnp.bfloat16)
        return carry

    lax.fori_loop(0, rows // conv_rows, conv_step, 0)

    locals_[2].wait()
    pairs = jnp.minimum(level, ring - 1 - level)

    def block_at(i):
        near = jnp.where(i % 2 == 1, level - (i + 1) // 2, level + i // 2)
        return jnp.where(i <= 2 * pairs, near, jnp.where(level < ring // 2, i, ring - 1 - i))

    group_cols = TEAM // 2 * wide
    jobs = [(i, h) for i in range(ring) for h in range(2)]

    def cols_of(j):
        i, h = jobs[j]
        return pl.ds(
            pl.multiple_of((block_at(i) * TEAM + h * (TEAM // 2)) * wide, group_cols), group_cols
        )

    ways = ((1, 2), (2, 1))

    def part_of(j, way):
        i, h = jobs[j]
        first = (block_at(i) * TEAM + h * (TEAM // 2)) * wide + way * wide
        return pl.ds(pl.multiple_of(first, wide), wide)

    many = TEAM * share
    half_many = many // 2

    def product(core, cols, store):
        def step(t, carry):
            at = pl.multiple_of(t * half_many, half_many)
            store(
                pl.ds(at, half_many),
                jnp.dot(
                    hid[pl.ds(pl.multiple_of(core * many + at, half_many), half_many)],
                    down_all[:, cols],
                    preferred_element_type=jnp.float32,
                ).astype(jnp.bfloat16),
            )
            return carry

        lax.fori_loop(0, 2, step, 0)

    twos, ones, seconds = {}, {}, {}

    def stage_product(j):
        i, h = jobs[j]
        if i >= 1:
            if i <= last:
                pass_on(2, i, h)
            else:
                receive(2, last, h)
        cols = cols_of(j)

        def away(at, part):
            psnd[j, at] = part

        def here(at, part):
            mine[j % 2, at] = part

        product(mate, cols, away)
        twos[j] = begin(remote(psnd.at[j], prcv.at[j], sum_s.at[0, j], sum_r.at[0, j], tp=mate))
        product(tp, cols, here)

    def shard(j, way, turn):
        at = pl.ds(pl.multiple_of(team_peer(place, turn) * share, share), share)
        cols = pl.ds(way * wide, wide)
        return mine[j % 2, at, cols].astype(jnp.float32) + prcv[j, at, cols].astype(jnp.float32)

    def stage_first(j):
        twos[j].wait_recv()
        for way, (one, two) in enumerate(ways):
            h1s[j, way, 0] = shard(j, way, one).astype(jnp.bfloat16)
            h1s[j, way, 1] = shard(j, way, 3).astype(jnp.bfloat16)
            sems = sum_s.at[1 + way, j], sum_r.at[1 + way, j]
            ones[j, way] = begin(remote(h1s.at[j, way], h1r.at[j, way], *sems, sp=peer(one)))
        for way, (one, two) in enumerate(ways):
            total[:, part_of(j, way)] = shard(j, way, 0)
            keep[j % 4, way] = shard(j, way, two)

    def stage_second(j):
        for way, (one, two) in enumerate(ways):
            ones[j, way].wait_recv()
            h2s[j, way] = (keep[j % 4, way] + h1r[j, way, 1].astype(jnp.float32)).astype(
                jnp.bfloat16
            )
            sems = sum_s.at[3 + way, j], sum_r.at[3 + way, j]
            seconds[j, way] = begin(remote(h2s.at[j, way], h2r.at[j, way], *sems, sp=peer(two)))
            total[:, part_of(j, way)] += h1r[j, way, 0].astype(jnp.float32)

    def stage_last(j):
        for way in range(2):
            seconds[j, way].wait_recv()
            total[:, part_of(j, way)] += h2r[j, way].astype(jnp.float32)

    stages = ((stage_last, 5), (stage_second, 3), (stage_first, 1), (stage_product, 0))
    for clock in range(len(jobs) + stages[0][1]):
        for stage, late in stages:
            if 0 <= clock - late < len(jobs):
                stage(clock - late)

    def out_step(t, carry):
        at = pl.ds(pl.multiple_of(t * band_rows, band_rows), band_rows)
        block = total[at]
        out_ref[at] = (mid[at] + block * row_scale(block) * gc_ref[...]).astype(out_ref.dtype)
        return carry

    lax.fori_loop(0, share // band_rows, out_step, 0)
    for there, copy in sends:
        if there is None:
            copy.wait_send()
        else:
            pl.when(there)(copy.wait_send)


def on_device_team(
    ring,
    queries,
    key_states,
    value_states,
    sink_logits,
    out_weight,
    residual,
    gain_attn,
    gain_before,
    gain_after,
    gate_weight,
    value_weight,
    gate_taps,
    value_taps,
    down_weight,
):
    length, width = queries.shape[0], residual.shape[1]
    share = residual.shape[0]
    wide, local_units = gate_weight.shape
    units = local_units // TEAM
    rows = length * TEAM
    edge = 16
    vmem = pl.BlockSpec(memory_space=pltpu.VMEM)
    smem = pl.BlockSpec(memory_space=pltpu.SMEM)
    far = pl.BlockSpec(memory_space=pl.ANY)
    dma = pltpu.SemaphoreType.DMA
    bf16, f32 = jnp.bfloat16, jnp.float32
    jobs, group_cols = ring * 2, TEAM // 2 * wide

    def buffer(*shape, dtype=bf16):
        return pltpu.VMEM(shape, dtype)

    return pl.pallas_call(
        functools.partial(layer_kernel, ring),
        out_shape=jax.ShapeDtypeStruct((share, width), bf16),
        in_specs=[vmem] * 3 + [smem] + [far] * 2 + [vmem] * 3 + [far] * 3 + [vmem] * 2,
        out_specs=vmem,
        scratch_shapes=[
            buffer(*out_weight.shape),
            buffer(share, width),
            buffer(share, width, dtype=f32),
            buffer(units, width),
            buffer(units, width),
            buffer(units, width),
            buffer(rows + edge, width),
            buffer(rows + edge, units),
            buffer(rows + edge, units),
            buffer(rows, units),
            buffer(2, 8, units, dtype=f32),
            buffer(length + WINDOW, key_states.shape[1]),
            buffer(length + WINDOW, key_states.shape[1]),
            buffer(*queries.shape),
            buffer(share, width),
            buffer(share, width),
            buffer(share, width),
            buffer(jobs, TEAM * share, group_cols),
            buffer(jobs, TEAM * share, group_cols),
            buffer(2, TEAM * share, group_cols),
            buffer(4, 2, share, wide, dtype=f32),
            buffer(jobs, 2, 2, share, wide),
            buffer(jobs, 2, 2, share, wide),
            buffer(jobs, 2, share, wide),
            buffer(jobs, 2, share, wide),
            buffer(share, width, dtype=f32),
            dma((2,)),
            dma((2,)),
            dma((3, TEAM - 1)),
            dma((3, TEAM - 1)),
            dma((5,)),
            dma((3, 2, TEAM)),
            dma((3, 2, TEAM)),
            dma((2, 2, ring - 2)),
            dma((2, 2, ring - 2)),
            dma((2, ring - 2, 2)),
            dma((2, ring - 2, 2)),
            dma(()),
            dma(()),
            dma((4,)),
            dma((4,)),
            dma((TEAM,)),
            dma((TEAM,)),
            dma(()),
            dma(()),
            dma((5, jobs)),
            dma((5, jobs)),
        ],
        compiler_params=pltpu.CompilerParams(
            collective_id=0, has_side_effects=True, vmem_limit_bytes=VMEM_BYTES
        ),
        name="layer",
    )(
        queries,
        key_states,
        value_states,
        sink_logits,
        out_weight,
        residual,
        gain_attn[None],
        gain_before[None],
        gain_after[None],
        gate_weight.T,
        value_weight.T,
        down_weight,
        gate_taps,
        value_taps,
    )


def solution(mesh):
    in_specs = (
        P("sp", "tp"),
        P("sp", "tp"),
        P("sp", "tp"),
        P("tp"),
        P("tp", None),
        P(("sp", "tp"), None),
        P(),
        P(),
        P(),
        P("sp", "tp"),
        P("sp", "tp"),
        P(None, "tp"),
        P(None, "tp"),
        P("tp", "sp"),
    )
    out_specs = P(("sp", "tp"), None)
    members, cores = mesh.shape["sp"], mesh.shape["tp"]
    ring = members // TEAM

    def on_device(*args):
        units, wide = args[13].shape
        teams = cores == 2 and members % TEAM == 0 and ring >= 3
        if teams and units % (TEAM * 16) == 0 and wide % 128 == 0:
            return on_device_team(ring, *args)
        return on_device_plain(*args)

    return jax.shard_map(
        on_device, mesh=mesh, in_specs=in_specs, out_specs=out_specs, check_vma=False
    )
```

```python
import functools

import jax
import jax.numpy as jnp
from jax import lax
from jax.experimental import pallas as pl
from jax.experimental.pallas import tpu as pltpu
from jax.sharding import PartitionSpec as P

HD = 64
WINDOW = 128
TEAM = 4


NEG_FILL = -1e30
MESH = pl.DeviceIdType.MESH
VMEM_BYTES = 63 * 1024 * 1024

def passed_along(block, axis, distance):
    devices = range(lax.axis_size(axis))
    route = [(i - distance, i) for i in devices if i - distance in devices]
    return lax.ppermute(block, axis, route)


def rms_scale(matrix):
    return matrix * lax.rsqrt(jnp.mean(matrix * matrix, axis=-1, keepdims=True) + 1e-06)


def attention_local(queries, key_states, value_states, sink_logits):
    length = queries.shape[0]
    blocks = length // WINDOW
    kv_local = key_states.shape[1] // HD
    grouping = queries.shape[1] // key_states.shape[1]
    earlier_keys, earlier_values = passed_along(
        (key_states[length - WINDOW :], value_states[length - WINDOW :]), "sp", 1
    )
    keys_ext = jnp.concatenate([earlier_keys, key_states], axis=0).reshape(
        blocks + 1, WINDOW, kv_local, HD
    )
    values_ext = jnp.concatenate([earlier_values, value_states], axis=0).reshape(
        blocks + 1, WINDOW, kv_local, HD
    )
    key_blocks = jnp.concatenate([keys_ext[:-1], keys_ext[1:]], axis=1)
    value_blocks = jnp.concatenate([values_ext[:-1], values_ext[1:]], axis=1)
    query_blocks = queries.reshape(blocks, WINDOW, kv_local, grouping, HD)
    offset = lax.axis_index("sp") * length
    qpos = (offset + jnp.arange(length, dtype=jnp.int32)).reshape(blocks, WINDOW)
    kpos = jnp.concatenate([qpos - WINDOW, qpos], axis=1)
    visible = (
        (kpos[:, None, :] <= qpos[:, :, None])
        & (qpos[:, :, None] - kpos[:, None, :] < WINDOW)
        & (kpos[:, None, :] >= 0)
    )
    scores = jnp.einsum(
        "nqhgd,nkhd->nhgqk", query_blocks, key_blocks, preferred_element_type=jnp.float32
    ) * HD ** (-0.5)
    scores = jnp.where(visible[:, None, None], scores, NEG_FILL)
    sink_col = sink_logits.reshape(kv_local, grouping)[None, :, :, None]
    top = jnp.maximum(jnp.max(scores, axis=-1), sink_col)
    expo = jnp.exp(scores - top[..., None])
    total = jnp.sum(expo, axis=-1) + jnp.exp(sink_col - top)
    probs = (expo / total[..., None]).astype(jnp.bfloat16)
    result = jnp.einsum(
        "nhgqk,nkhd->nqhgd", probs, value_blocks, preferred_element_type=jnp.float32
    )
    return result.astype(jnp.bfloat16).reshape(length, queries.shape[1])


def causal_local(upward, earlier, kernel):
    length = upward.shape[0]
    padded = jnp.concatenate([earlier, upward], axis=0).astype(jnp.float32)
    result = jnp.zeros(upward.shape, jnp.float32)
    for tap_index in range(kernel.shape[0]):
        result = result + kernel[tap_index][None, :] * padded[tap_index : tap_index + length]
    return result


def on_device_plain(
    queries,
    key_states,
    value_states,
    sink_logits,
    out_weight,
    residual,
    gain_attn,
    gain_before,
    gain_after,
    gate_weight,
    value_weight,
    gate_taps,
    value_taps,
    down_weight,
):
    length = queries.shape[0]
    attended = attention_local(queries, key_states, value_states, sink_logits)
    selected = attended
    attn_proj = lax.psum_scatter(
        jnp.dot(selected, out_weight, preferred_element_type=jnp.float32).astype(jnp.bfloat16),
        "tp",
        scatter_dimension=0,
        tiled=True,
    ).astype(jnp.float32)
    middle = residual.astype(jnp.float32) + rms_scale(attn_proj) * gain_attn
    normed = (rms_scale(middle) * gain_before).astype(jnp.bfloat16)
    whole_rows = lax.all_gather(normed, "tp", axis=0, tiled=True)
    gate_full, value_full = (
        lax.all_gather(gate_weight, "sp", axis=0, tiled=True),
        lax.all_gather(value_weight, "sp", axis=0, tiled=True),
    )
    gate_up = jnp.dot(whole_rows, gate_full, preferred_element_type=jnp.float32).astype(
        jnp.bfloat16
    )
    value_up = jnp.dot(whole_rows, value_full, preferred_element_type=jnp.float32).astype(
        jnp.bfloat16
    )
    reach = gate_taps.shape[0] - 1
    gate_before, value_before = passed_along(
        (gate_up[length - reach :], value_up[length - reach :]), "sp", 1
    )
    gate_conv = causal_local(gate_up, gate_before, gate_taps)
    value_conv = causal_local(value_up, value_before, value_taps)
    hidden = (jax.nn.silu(gate_conv) * value_conv).astype(jnp.bfloat16)
    down_whole = lax.all_gather(down_weight, "sp", axis=1, tiled=True)
    selected = hidden
    down = lax.psum_scatter(
        jnp.dot(selected, down_whole, preferred_element_type=jnp.float32).astype(jnp.bfloat16),
        "tp",
        scatter_dimension=0,
        tiled=True,
    ).astype(jnp.float32)
    return (middle + rms_scale(down) * gain_after).astype(jnp.bfloat16)


def team_peer(place, turn):
    low, high = place % 2, place // 2
    if turn & 1:
        low = 1 - low
    if turn & 2:
        high = 1 - high
    return high * 2 + low


def remote(src, dst, send, recv, **device):
    return pltpu.make_async_remote_copy(
        src_ref=src, dst_ref=dst, send_sem=send, recv_sem=recv, device_id=device, device_id_type=MESH
    )


def row_scale(block):
    return lax.rsqrt(jnp.mean(block * block, axis=-1, keepdims=True) + 1e-06)


def rows_by_units(rows, weight):
    return lax.dot_general(
        rows, weight, (((1,), (1,)), ((), ())), preferred_element_type=jnp.float32
    )


def even_parts(total, wanted):
    for parts in range(wanted, 0, -1):
        if total % (parts * 16) == 0:
            return parts


def unit_parts(units):
    return [(first, min(256, units - first)) for first in range(0, units, 256)]


def layer_kernel(
    ring,
    q_far,
    k_ref,
    v_ref,
    sink_ref,
    ow_far,
    res_far,
    ga_ref,
    gb_ref,
    gc_ref,
    gate_far,
    value_far,
    down_far,
    gate_taps,
    value_taps,
    out_ref,
    q_ref,
    ow,
    res,
    mid,
    gate_all,
    value_all,
    down_all,
    rows_all,
    gate_up,
    value_up,
    hid,
    taps,
    k_ext,
    v_ext,
    att,
    snd,
    rcv,
    own,
    psnd,
    prcv,
    mine,
    keep,
    h1s,
    h1r,
    h2s,
    h2r,
    total,
    halo_s,
    halo_r,
    trade_s,
    trade_r,
    local_sem,
    first_s,
    first_r,
    next_s,
    next_r,
    half_s,
    half_r,
    pair_s,
    pair_r,
    rows_s,
    rows_r,
    mate_s,
    mate_r,
    edge_s,
    edge_r,
    sum_s,
    sum_r,
):
    sp, tp = lax.axis_index("sp"), lax.axis_index("tp")
    members = ring * TEAM
    level, place = sp // TEAM, sp % TEAM
    mate = 1 - tp
    length = q_ref.shape[0]
    share = length // 2
    units = gate_all.shape[0]
    wide = gate_far.shape[1]
    last = ring - 2
    parts = unit_parts(units)
    cuts = ((0, 2), (2, 1), (3, 1))
    sends = []

    def peer(turn):
        return level * TEAM + team_peer(place, turn)

    has_up, has_down = level < ring - 1, level > 0
    has_after, has_before = sp < members - 1, sp > 0

    barrier = pltpu.get_barrier_semaphore()

    def greet(**device):
        pl.semaphore_signal(barrier, inc=1, device_id=device, device_id_type=MESH)

    greet(tp=mate)
    for turn in (1, 2, 3):
        greet(sp=peer(turn))
    pl.when(has_up)(lambda: greet(sp=sp + TEAM))
    pl.when(has_down)(lambda: greet(sp=sp - TEAM))
    pl.when(has_after)(lambda: greet(sp=sp + 1))
    pl.when(has_before)(lambda: greet(sp=sp - 1))
    others = sum(jnp.where(there, 1, 0) for there in (has_up, has_down, has_after, has_before))
    pl.semaphore_wait(barrier, TEAM + others)

    def begin(copy, there=None):
        if there is None:
            copy.start()
        else:
            pl.when(there)(copy.start)
        sends.append((there, copy))
        return copy

    def arrive(copy, there=None):
        if there is None:
            copy.wait_recv()
        else:
            pl.when(there)(copy.wait_recv)

    halos = [
        begin(
            remote(
                ref.at[pl.ds(length - WINDOW, WINDOW)],
                ext.at[pl.ds(0, WINDOW)],
                halo_s.at[i],
                halo_r.at[i],
                sp=sp + 1,
            ),
            has_after,
        )
        for i, (ref, ext) in enumerate(((k_ref, k_ext), (v_ref, v_ext)))
    ]

    fars = (gate_far, value_far, down_far)
    wholes = (gate_all, value_all, down_all)

    def span(m, start, size):
        return wholes[m].at[:, pl.ds(pl.multiple_of(start * wide, wide), size * wide)]

    def piece(m, member):
        return fars[m].at[pl.ds(pl.multiple_of(member * units, units), units)]

    def can_send(side, step):
        return has_up & (level >= step) if side == 0 else has_down & (level + step < ring)

    def can_receive(side, step):
        return level > step if side == 0 else level + step < ring - 1

    def toward(side):
        return sp + TEAM if side == 0 else sp - TEAM

    def first_copy(m, side, q, source=None):
        block = span(m, level * TEAM + q, 1)
        return remote(
            block if source is None else source,
            block,
            first_s.at[m, side, q],
            first_r.at[m, side, q],
            sp=toward(side),
        )

    def next_copy(m, side, step, block, half=None):
        if m == 0:
            part = span(m, block * TEAM, TEAM)
            sems = next_s.at[0, side, step - 1], next_r.at[0, side, step - 1]
        elif m == 1:
            first, size = parts[half]
            part = span(m, block * TEAM, TEAM).at[pl.ds(first, size)]
            sems = next_s.at[1 + half, side, step - 1], next_r.at[1 + half, side, step - 1]
        else:
            first, size = cuts[half]
            part = span(m, block * TEAM + first, size)
            sems = half_s.at[side, step - 1, half], half_r.at[side, step - 1, half]
        return remote(part, part, *sems, sp=toward(side))

    def came(side, step):
        return level - 1 - step if side == 0 else level + 1 + step

    def receive(m, step, half=None):
        for side in range(2):
            there = can_receive(side, step)
            if step == 0:
                members_in = range(TEAM)
                if m == 2:
                    members_in = range(cuts[half][0], sum(cuts[half]))
                for q in members_in:
                    block = span(m, came(side, 0) * TEAM + q, 1)
                    sems = first_s.at[m, side, q], first_r.at[m, side, q]
                    arrive(remote(block, block, *sems, sp=toward(side)), there)
            else:
                arrive(next_copy(m, side, step, came(side, step), half), there)

    def pass_on(m, step, half=None):
        if not (m == 1 and step == 1 and half):
            receive(m, step - 1, half)
        for side in range(2):
            block = level - step if side == 0 else level + step
            begin(next_copy(m, side, step, block, half), can_send(side, step))

    def own_first(m):
        for side in range(2):
            begin(first_copy(m, side, place, piece(m, place)), can_send(side, 0))

    trades, locals_ = [], []
    for m in range(3):
        trades.append(
            {
                turn: begin(
                    remote(
                        piece(m, team_peer(place, turn)),
                        span(m, sp, 1),
                        trade_s.at[m, turn - 1],
                        trade_r.at[m, turn - 1],
                        sp=peer(turn),
                    )
                )
                for turn in (1, 2, 3)
            }
        )
        own_first(m)
        copy = pltpu.make_async_copy(piece(m, place), span(m, sp, 1), local_sem.at[m])
        copy.start()
        locals_.append(copy)
    fetch_q = pltpu.make_async_copy(q_far, q_ref, local_sem.at[5])
    fetch_q.start()
    fetch_kv = [
        pltpu.make_async_copy(ref, ext.at[pl.ds(WINDOW, length)], local_sem.at[6 + i])
        for i, (ref, ext) in enumerate(((k_ref, k_ext), (v_ref, v_ext)))
    ]
    for copy in fetch_kv:
        copy.start()
    fetch_ow = pltpu.make_async_copy(ow_far, ow, local_sem.at[3])
    fetch_ow.start()
    fetch_res = pltpu.make_async_copy(res_far, res, local_sem.at[4])
    fetch_res.start()

    def first_rest(m):
        for turn in (1, 2, 3):
            trades[m][turn].wait_recv()
            for side in range(2):
                begin(first_copy(m, side, team_peer(place, turn)), can_send(side, 0))

    def down_rest():
        for q in range(TEAM):
            turn = jnp.abs(place % 2 - q % 2) + 2 * jnp.abs(place // 2 - q // 2)

            @pl.when(turn > 0)
            def _(q=q, turn=turn):
                block = span(2, level * TEAM + q, 1)
                sems = trade_s.at[2, turn - 1], trade_r.at[2, turn - 1]
                remote(block, block, *sems, sp=level * TEAM + q).wait_recv()

            for side in range(2):
                begin(first_copy(2, side, q), can_send(side, 0) & (turn > 0))

    pending = [
        (m, step, part)
        for step in range(1, last + 1)
        for m in range(2)
        for part in (range(len(parts)) if m else (None,))
    ]

    def pass_next(count):
        for m, step, part in pending[:count]:
            pass_on(m, step, part)
        del pending[:count]

    @pl.when(jnp.logical_not(has_before))
    def _():
        k_ext[pl.ds(0, WINDOW)] = jnp.zeros((WINDOW, k_ref.shape[1]), k_ref.dtype)
        v_ext[pl.ds(0, WINDOW)] = jnp.zeros((WINDOW, k_ref.shape[1]), k_ref.dtype)

    for p in range(TEAM):

        @pl.when(place == p)
        def _(p=p):
            for i, ref in enumerate((gate_taps, value_taps)):
                taps[i, : ref.shape[0]] = ref[:, p * units : (p + 1) * units]

    first_rest(0)
    for copy in halos:
        arrive(copy, has_before)
    fetch_q.wait()
    for copy in fetch_kv:
        copy.wait()
    heads_kv = k_ref.shape[1] // HD
    grouping = q_ref.shape[1] // k_ref.shape[1]
    row = lax.broadcasted_iota(jnp.int32, (WINDOW, 2 * WINDOW), 0)
    col = lax.broadcasted_iota(jnp.int32, (WINDOW, 2 * WINDOW), 1)
    band = (col <= row + WINDOW) & (col > row)

    for kv in range(heads_kv):

        def block_step(n, carry, kv=kv):
            start = pl.multiple_of(n * WINDOW, WINDOW)
            keys = k_ext[pl.ds(start, 2 * WINDOW), kv * HD : (kv + 1) * HD]
            values = v_ext[pl.ds(start, 2 * WINDOW), kv * HD : (kv + 1) * HD]
            wide_q = q_ref[pl.ds(start, WINDOW), kv * grouping * HD : (kv + 1) * grouping * HD]
            visible = band & (col + (sp * length + start - WINDOW) >= 0)
            stacked = jnp.concatenate(
                [wide_q[:, g * HD : (g + 1) * HD] for g in range(grouping)], axis=0
            )
            scores = lax.dot_general(
                stacked, keys, (((1,), (1,)), ((), ())), preferred_element_type=jnp.float32
            ) * HD ** (-0.5)
            probs = []
            for g in range(grouping):
                sink = sink_ref[kv * grouping + g]
                part = jnp.where(visible, scores[g * WINDOW : (g + 1) * WINDOW], NEG_FILL)
                top = jnp.maximum(jnp.max(part, axis=-1, keepdims=True), sink)
                expo = jnp.exp(part - top)
                whole = jnp.sum(expo, axis=-1, keepdims=True) + jnp.exp(sink - top)
                probs.append((expo / whole).astype(jnp.bfloat16))
            result = jnp.dot(
                jnp.concatenate(probs, axis=0), values, preferred_element_type=jnp.float32
            ).astype(jnp.bfloat16)
            att[pl.ds(start, WINDOW), kv * grouping * HD : (kv + 1) * grouping * HD] = (
                jnp.concatenate(
                    [result[g * WINDOW : (g + 1) * WINDOW] for g in range(grouping)], axis=1
                )
            )
            return carry

        lax.fori_loop(0, length // WINDOW, block_step, 0)
        if kv == 0:
            first_rest(1)

    columns = ow.shape[1]
    tile = min(512, columns)
    fetch_ow.wait()

    def project(rows_start, target):
        def tile_step(t, carry):
            at = pl.multiple_of(t * tile, tile)
            target[:, pl.ds(at, tile)] = jnp.dot(
                att[pl.ds(rows_start, share)],
                ow[:, pl.ds(at, tile)],
                preferred_element_type=jnp.float32,
            ).astype(jnp.bfloat16)
            return carry

        lax.fori_loop(0, columns // tile, tile_step, 0)

    project(pl.multiple_of(mate * share, share), snd)
    pair = begin(remote(snd, rcv, pair_s, pair_r, tp=mate))
    project(pl.multiple_of(tp * share, share), own)
    fetch_res.wait()
    pair.wait_recv()
    band_rows = 32
    rows = length * TEAM
    edge = rows_all.shape[0] - rows

    def row_start(member, core):
        return pl.multiple_of(edge + (member * 2 + core) * share, edge)

    my_rows = row_start(place, tp)

    def norm_step(t, carry):
        at = pl.ds(pl.multiple_of(t * band_rows, band_rows), band_rows)
        proj = own[at].astype(jnp.float32) + rcv[at].astype(jnp.float32)
        middle = res[at].astype(jnp.float32) + proj * row_scale(proj) * ga_ref[...]
        mid[at] = middle
        rows_all[pl.ds(pl.multiple_of(my_rows + t * band_rows, edge), band_rows)] = (
            middle * row_scale(middle) * gb_ref[...]
        ).astype(jnp.bfloat16)
        return carry

    lax.fori_loop(0, share // band_rows, norm_step, 0)

    def slot(member, first=0, size=share):
        start = pl.multiple_of(row_start(member, tp) + first, edge)
        return rows_all.at[pl.ds(start, size)]

    def row_copy(block, i, turn):
        return begin(remote(block, block, rows_s.at[i], rows_r.at[i], sp=peer(turn)))

    def to_mate(block, i):
        return begin(remote(block, block, mate_s.at[i], mate_r.at[i], tp=mate))

    half = share // 2
    mine_rows = slot(place)
    across = [row_copy(mine_rows, 0, 1), row_copy(mine_rows, 1, 2)]
    mates = [to_mate(mine_rows, 0)]
    pass_next(1)
    pass_next(len(parts))
    across[0].wait_recv()
    across.append(row_copy(slot(team_peer(place, 1), 0, half), 2, 2))
    mates.append(to_mate(slot(team_peer(place, 1)), 1))
    across[1].wait_recv()
    across.append(row_copy(slot(team_peer(place, 2), half, half), 3, 1))
    mates.append(to_mate(slot(team_peer(place, 2)), 2))
    pass_next(1)
    across[2].wait_recv()
    across[3].wait_recv()
    mates.append(to_mate(slot(team_peer(place, 3)), 3))
    for copy in mates:
        copy.wait_recv()
    ending = remote(
        rows_all.at[pl.ds(rows, edge)], rows_all.at[pl.ds(0, edge)], edge_s, edge_r, sp=sp + TEAM
    )
    begin(ending, has_up)

    @pl.when(jnp.logical_not(has_down))
    def _():
        rows_all[pl.ds(0, edge)] = jnp.zeros((edge, rows_all.shape[1]), rows_all.dtype)

    pass_next(len(pending))
    arrive(ending, has_down)

    steps = even_parts(rows + edge, 4)
    chunk = (rows + edge) // steps

    def up(m, result, first=0, size=units):
        def up_step(t, carry):
            at = pl.ds(pl.multiple_of(t * chunk, edge), chunk)
            result[at, first : first + size] = rows_by_units(
                rows_all[at], wholes[m][first : first + size]
            ).astype(jnp.bfloat16)
            return carry

        lax.fori_loop(0, steps, up_step, 0)

    receive(0, last)
    locals_[0].wait()
    up(0, gate_up)
    down_rest()
    locals_[1].wait()
    reach = gate_taps.shape[0] - 1
    conv_rows = 64
    per = share // conv_rows

    def conv_step(t, carry, first_unit, size):
        unit_span = slice(first_unit, first_unit + size)
        at = pl.multiple_of(t * conv_rows, conv_rows)

        def mixed(source, i):
            padded = source[pl.ds(at, conv_rows + edge), unit_span].astype(jnp.float32)
            result = jnp.zeros((conv_rows, size), jnp.float32)
            for k in range(reach + 1):
                first = edge - reach + k
                result = result + taps[i, k : k + 1, unit_span] * padded[first : first + conv_rows]
            return result

        gate = mixed(gate_up, 0)
        value = mixed(value_up, 1)
        group = t // per
        to = (group % 2 * TEAM + group // 2) * share + t % per * conv_rows
        hid[pl.ds(pl.multiple_of(to, conv_rows), conv_rows), unit_span] = (
            gate / (1.0 + jnp.exp(-gate)) * value
        ).astype(jnp.bfloat16)
        return carry

    for i, (first_unit, size) in enumerate(parts):
        receive(1, last, i)
        up(1, value_up, first_unit, size)
        mixing = functools.partial(conv_step, first_unit=first_unit, size=size)
        lax.fori_loop(0, rows // conv_rows, mixing, 0)

    locals_[2].wait()
    pairs = jnp.minimum(level, ring - 1 - level)

    def block_at(i):
        near = jnp.where(i % 2 == 1, level - (i + 1) // 2, level + i // 2)
        return jnp.where(i <= 2 * pairs, near, jnp.where(level < ring // 2, i, ring - 1 - i))

    jobs = [(i, *job) for i in range(ring - 1) for job in ((0, 2, (0,)), (2, 2, (1, 2)))]
    jobs += [(ring - 1, *cut, (i,)) for i, cut in enumerate(cuts)]

    def cols_of(j):
        i, first, size, _ = jobs[j]
        at = pl.multiple_of((block_at(i) * TEAM + first) * wide, size * wide)
        return pl.ds(at, size * wide)

    def width_of(j):
        return slice(0, jobs[j][2] * wide)

    ways = ((1, 2), (2, 1))

    def part_of(way):
        return slice(way * half, (way + 1) * half)

    many = TEAM * share
    half_many = many // 2

    def product(core, cols, store):
        def step(t, carry):
            at = pl.multiple_of(t * half_many, half_many)
            store(
                pl.ds(at, half_many),
                jnp.dot(
                    hid[pl.ds(pl.multiple_of(core * many + at, half_many), half_many)],
                    down_all[:, cols],
                    preferred_element_type=jnp.float32,
                ).astype(jnp.bfloat16),
            )
            return carry

        lax.fori_loop(0, 2, step, 0)

    twos, ones, seconds = {}, {}, {}

    def stage_product(j):
        i, needed = jobs[j][0], jobs[j][3]
        if i >= 1:
            for cut in needed:
                if i <= last:
                    pass_on(2, i, cut)
                else:
                    receive(2, last, cut)
        cols = cols_of(j)

        def away(at, part):
            psnd[j, at, width_of(j)] = part

        def here(at, part):
            mine[j % 2, at, width_of(j)] = part

        product(mate, cols, away)
        there = (j, slice(None), width_of(j))
        sems = sum_s.at[0, j], sum_r.at[0, j]
        twos[j] = begin(remote(psnd.at[*there], prcv.at[*there], *sems, tp=mate))
        product(tp, cols, here)

    def shard(j, way, turn):
        at = pl.ds(pl.multiple_of(team_peer(place, turn) * share + way * half, half), half)
        cols = width_of(j)
        return mine[j % 2, at, cols].astype(jnp.float32) + prcv[j, at, cols].astype(jnp.float32)

    def stage_first(j):
        twos[j].wait_recv()
        cols = width_of(j)
        for way, (one, two) in enumerate(ways):
            h1s[j, way, 0, :, cols] = shard(j, way, one).astype(jnp.bfloat16)
            h1s[j, way, 1, :, cols] = shard(j, way, 3).astype(jnp.bfloat16)
            there = (j, way, slice(None), slice(None), cols)
            sems = sum_s.at[1 + way, j], sum_r.at[1 + way, j]
            ones[j, way] = begin(remote(h1s.at[*there], h1r.at[*there], *sems, sp=peer(one)))
        for way, (one, two) in enumerate(ways):
            total[part_of(way), cols_of(j)] = shard(j, way, 0)
            keep[j % 4, way, :, cols] = shard(j, way, two)

    def stage_second(j):
        cols = width_of(j)
        for way, (one, two) in enumerate(ways):
            ones[j, way].wait_recv()
            h2s[j, way, :, cols] = (
                keep[j % 4, way, :, cols] + h1r[j, way, 1, :, cols].astype(jnp.float32)
            ).astype(jnp.bfloat16)
            there = (j, way, slice(None), cols)
            sems = sum_s.at[3 + way, j], sum_r.at[3 + way, j]
            seconds[j, way] = begin(remote(h2s.at[*there], h2r.at[*there], *sems, sp=peer(two)))
            total[part_of(way), cols_of(j)] += h1r[j, way, 0, :, cols].astype(jnp.float32)

    def stage_last(j):
        cols = width_of(j)
        for way in range(2):
            seconds[j, way].wait_recv()
            total[part_of(way), cols_of(j)] += h2r[j, way, :, cols].astype(jnp.float32)

    stages = ((stage_last, 5), (stage_second, 3), (stage_first, 1), (stage_product, 0))
    for clock in range(len(jobs) + stages[0][1]):
        for stage, late in stages:
            if 0 <= clock - late < len(jobs):
                stage(clock - late)

    def out_step(t, carry):
        at = pl.ds(pl.multiple_of(t * band_rows, band_rows), band_rows)
        block = total[at]
        out_ref[at] = (mid[at] + block * row_scale(block) * gc_ref[...]).astype(out_ref.dtype)
        return carry

    lax.fori_loop(0, share // band_rows, out_step, 0)
    for there, copy in sends:
        if there is None:
            copy.wait_send()
        else:
            pl.when(there)(copy.wait_send)


def on_device_team(
    ring,
    queries,
    key_states,
    value_states,
    sink_logits,
    out_weight,
    residual,
    gain_attn,
    gain_before,
    gain_after,
    gate_weight,
    value_weight,
    gate_taps,
    value_taps,
    down_weight,
):
    length, width = queries.shape[0], residual.shape[1]
    share = residual.shape[0]
    wide, local_units = gate_weight.shape
    units = local_units // TEAM
    rows = length * TEAM
    edge = 16
    vmem = pl.BlockSpec(memory_space=pltpu.VMEM)
    smem = pl.BlockSpec(memory_space=pltpu.SMEM)
    far = pl.BlockSpec(memory_space=pl.ANY)
    dma = pltpu.SemaphoreType.DMA
    bf16, f32 = jnp.bfloat16, jnp.float32
    jobs, group_cols = ring * 2 + 1, TEAM // 2 * wide

    def buffer(*shape, dtype=bf16):
        return pltpu.VMEM(shape, dtype)

    return pl.pallas_call(
        functools.partial(layer_kernel, ring),
        out_shape=jax.ShapeDtypeStruct((share, width), bf16),
        in_specs=[far] * 3 + [smem] + [far] * 2 + [vmem] * 3 + [far] * 3 + [vmem] * 2,
        out_specs=vmem,
        scratch_shapes=[
            buffer(*queries.shape),
            buffer(*out_weight.shape),
            buffer(share, width),
            buffer(share, width, dtype=f32),
            buffer(units, width),
            buffer(units, width),
            buffer(units, width),
            buffer(rows + edge, width),
            buffer(rows + edge, units),
            buffer(rows + edge, units),
            buffer(rows, units),
            buffer(2, 8, units, dtype=f32),
            buffer(length + WINDOW, key_states.shape[1]),
            buffer(length + WINDOW, key_states.shape[1]),
            buffer(*queries.shape),
            buffer(share, width),
            buffer(share, width),
            buffer(share, width),
            buffer(jobs, TEAM * share, group_cols),
            buffer(jobs, TEAM * share, group_cols),
            buffer(2, TEAM * share, group_cols),
            buffer(4, 2, share // 2, group_cols, dtype=f32),
            buffer(jobs, 2, 2, share // 2, group_cols),
            buffer(jobs, 2, 2, share // 2, group_cols),
            buffer(jobs, 2, share // 2, group_cols),
            buffer(jobs, 2, share // 2, group_cols),
            buffer(share, width, dtype=f32),
            dma((2,)),
            dma((2,)),
            dma((3, TEAM - 1)),
            dma((3, TEAM - 1)),
            dma((8,)),
            dma((3, 2, TEAM)),
            dma((3, 2, TEAM)),
            dma((1 + len(unit_parts(units)), 2, ring - 2)),
            dma((1 + len(unit_parts(units)), 2, ring - 2)),
            dma((2, ring - 2, 3)),
            dma((2, ring - 2, 3)),
            dma(()),
            dma(()),
            dma((4,)),
            dma((4,)),
            dma((TEAM,)),
            dma((TEAM,)),
            dma(()),
            dma(()),
            dma((5, jobs)),
            dma((5, jobs)),
        ],
        compiler_params=pltpu.CompilerParams(
            collective_id=0, has_side_effects=True, vmem_limit_bytes=VMEM_BYTES
        ),
        name="layer",
    )(
        queries,
        key_states,
        value_states,
        sink_logits,
        out_weight,
        residual,
        gain_attn[None],
        gain_before[None],
        gain_after[None],
        gate_weight.T,
        value_weight.T,
        down_weight,
        gate_taps,
        value_taps,
    )


def solution(mesh):
    in_specs = (
        P("sp", "tp"),
        P("sp", "tp"),
        P("sp", "tp"),
        P("tp"),
        P("tp", None),
        P(("sp", "tp"), None),
        P(),
        P(),
        P(),
        P("sp", "tp"),
        P("sp", "tp"),
        P(None, "tp"),
        P(None, "tp"),
        P("tp", "sp"),
    )
    out_specs = P(("sp", "tp"), None)
    members, cores = mesh.shape["sp"], mesh.shape["tp"]
    ring = members // TEAM

    def on_device(*args):
        units, wide = args[13].shape
        teams = cores == 2 and members % TEAM == 0 and ring >= 3
        if teams and units % (TEAM * 16) == 0 and wide % 128 == 0:
            return on_device_team(ring, *args)
        return on_device_plain(*args)

    return jax.shard_map(
        on_device, mesh=mesh, in_specs=in_specs, out_specs=out_specs, check_vma=False
    )
```

```python
import functools

import jax
import jax.numpy as jnp
from jax import lax
from jax.experimental import pallas as pl
from jax.experimental.pallas import tpu as pltpu
from jax.sharding import PartitionSpec as P

HD = 64
WINDOW = 128
TEAM = 4


NEG_FILL = -1e30
MESH = pl.DeviceIdType.MESH
VMEM_BYTES = 63 * 1024 * 1024

def passed_along(block, axis, distance):
    devices = range(lax.axis_size(axis))
    route = [(i - distance, i) for i in devices if i - distance in devices]
    return lax.ppermute(block, axis, route)


def rms_scale(matrix):
    return matrix * lax.rsqrt(jnp.mean(matrix * matrix, axis=-1, keepdims=True) + 1e-06)


def attention_local(queries, key_states, value_states, sink_logits):
    length = queries.shape[0]
    blocks = length // WINDOW
    kv_local = key_states.shape[1] // HD
    grouping = queries.shape[1] // key_states.shape[1]
    earlier_keys, earlier_values = passed_along(
        (key_states[length - WINDOW :], value_states[length - WINDOW :]), "sp", 1
    )
    keys_ext = jnp.concatenate([earlier_keys, key_states], axis=0).reshape(
        blocks + 1, WINDOW, kv_local, HD
    )
    values_ext = jnp.concatenate([earlier_values, value_states], axis=0).reshape(
        blocks + 1, WINDOW, kv_local, HD
    )
    key_blocks = jnp.concatenate([keys_ext[:-1], keys_ext[1:]], axis=1)
    value_blocks = jnp.concatenate([values_ext[:-1], values_ext[1:]], axis=1)
    query_blocks = queries.reshape(blocks, WINDOW, kv_local, grouping, HD)
    offset = lax.axis_index("sp") * length
    qpos = (offset + jnp.arange(length, dtype=jnp.int32)).reshape(blocks, WINDOW)
    kpos = jnp.concatenate([qpos - WINDOW, qpos], axis=1)
    visible = (
        (kpos[:, None, :] <= qpos[:, :, None])
        & (qpos[:, :, None] - kpos[:, None, :] < WINDOW)
        & (kpos[:, None, :] >= 0)
    )
    scores = jnp.einsum(
        "nqhgd,nkhd->nhgqk", query_blocks, key_blocks, preferred_element_type=jnp.float32
    ) * HD ** (-0.5)
    scores = jnp.where(visible[:, None, None], scores, NEG_FILL)
    sink_col = sink_logits.reshape(kv_local, grouping)[None, :, :, None]
    top = jnp.maximum(jnp.max(scores, axis=-1), sink_col)
    expo = jnp.exp(scores - top[..., None])
    total = jnp.sum(expo, axis=-1) + jnp.exp(sink_col - top)
    probs = (expo / total[..., None]).astype(jnp.bfloat16)
    result = jnp.einsum(
        "nhgqk,nkhd->nqhgd", probs, value_blocks, preferred_element_type=jnp.float32
    )
    return result.astype(jnp.bfloat16).reshape(length, queries.shape[1])


def causal_local(upward, earlier, kernel):
    length = upward.shape[0]
    padded = jnp.concatenate([earlier, upward], axis=0).astype(jnp.float32)
    result = jnp.zeros(upward.shape, jnp.float32)
    for tap_index in range(kernel.shape[0]):
        result = result + kernel[tap_index][None, :] * padded[tap_index : tap_index + length]
    return result


def on_device_plain(
    queries,
    key_states,
    value_states,
    sink_logits,
    out_weight,
    residual,
    gain_attn,
    gain_before,
    gain_after,
    gate_weight,
    value_weight,
    gate_taps,
    value_taps,
    down_weight,
):
    length = queries.shape[0]
    attended = attention_local(queries, key_states, value_states, sink_logits)
    selected = attended
    attn_proj = lax.psum_scatter(
        jnp.dot(selected, out_weight, preferred_element_type=jnp.float32).astype(jnp.bfloat16),
        "tp",
        scatter_dimension=0,
        tiled=True,
    ).astype(jnp.float32)
    middle = residual.astype(jnp.float32) + rms_scale(attn_proj) * gain_attn
    normed = (rms_scale(middle) * gain_before).astype(jnp.bfloat16)
    whole_rows = lax.all_gather(normed, "tp", axis=0, tiled=True)
    gate_full, value_full = (
        lax.all_gather(gate_weight, "sp", axis=0, tiled=True),
        lax.all_gather(value_weight, "sp", axis=0, tiled=True),
    )
    gate_up = jnp.dot(whole_rows, gate_full, preferred_element_type=jnp.float32).astype(
        jnp.bfloat16
    )
    value_up = jnp.dot(whole_rows, value_full, preferred_element_type=jnp.float32).astype(
        jnp.bfloat16
    )
    reach = gate_taps.shape[0] - 1
    gate_before, value_before = passed_along(
        (gate_up[length - reach :], value_up[length - reach :]), "sp", 1
    )
    gate_conv = causal_local(gate_up, gate_before, gate_taps)
    value_conv = causal_local(value_up, value_before, value_taps)
    hidden = (jax.nn.silu(gate_conv) * value_conv).astype(jnp.bfloat16)
    down_whole = lax.all_gather(down_weight, "sp", axis=1, tiled=True)
    selected = hidden
    down = lax.psum_scatter(
        jnp.dot(selected, down_whole, preferred_element_type=jnp.float32).astype(jnp.bfloat16),
        "tp",
        scatter_dimension=0,
        tiled=True,
    ).astype(jnp.float32)
    return (middle + rms_scale(down) * gain_after).astype(jnp.bfloat16)


def team_peer(place, turn):
    low, high = place % 2, place // 2
    if turn & 1:
        low = 1 - low
    if turn & 2:
        high = 1 - high
    return high * 2 + low


def remote(src, dst, send, recv, **device):
    return pltpu.make_async_remote_copy(
        src_ref=src, dst_ref=dst, send_sem=send, recv_sem=recv, device_id=device, device_id_type=MESH
    )


def row_scale(block):
    return lax.rsqrt(jnp.mean(block * block, axis=-1, keepdims=True) + 1e-06)


def rows_by_units(rows, weight):
    return lax.dot_general(
        rows, weight, (((1,), (1,)), ((), ())), preferred_element_type=jnp.float32
    )


def even_parts(total, wanted):
    for parts in range(wanted, 0, -1):
        if total % (parts * 16) == 0:
            return parts


def unit_parts(units):
    return [(first, min(256, units - first)) for first in range(0, units, 256)]


def layer_kernel(
    ring,
    q_far,
    k_ref,
    v_ref,
    sink_ref,
    ow_far,
    res_far,
    ga_ref,
    gb_ref,
    gc_ref,
    gate_far,
    value_far,
    down_far,
    gate_taps,
    value_taps,
    out_ref,
    q_ref,
    ow,
    res,
    mid,
    gate_all,
    value_all,
    down_all,
    rows_all,
    gate_up,
    value_up,
    hid,
    taps,
    k_ext,
    v_ext,
    att,
    snd,
    rcv,
    own,
    psnd,
    prcv,
    mine,
    keep,
    h1s,
    h1r,
    h2s,
    h2r,
    total,
    halo_s,
    halo_r,
    trade_s,
    trade_r,
    local_sem,
    first_s,
    first_r,
    next_s,
    next_r,
    half_s,
    half_r,
    pair_s,
    pair_r,
    rows_s,
    rows_r,
    mate_s,
    mate_r,
    edge_s,
    edge_r,
    sum_s,
    sum_r,
    raw_sem,
):
    sp, tp = lax.axis_index("sp"), lax.axis_index("tp")
    members = ring * TEAM
    level, place = sp // TEAM, sp % TEAM
    mate = 1 - tp
    length = q_ref.shape[0]
    share = length // 2
    units = gate_all.shape[0]
    wide, deep = down_far.shape[1], gate_far.shape[0]
    last = ring - 2
    parts = unit_parts(units)
    cuts = ((0, 2), (2, 1), (3, 1))
    sends = []

    def peer(turn):
        return level * TEAM + team_peer(place, turn)

    group = psnd.shape[2]
    stacked_raw = psnd.shape[1] // deep

    def raw_piece(m, i):
        at = pl.ds(i % stacked_raw * deep, deep)
        return psnd.at[2 * m + i // stacked_raw, at]

    raws = [
        [
            pltpu.make_async_copy(
                ref.at[:, pl.ds(i * group, group)], raw_piece(m, i), raw_sem.at[m, i]
            )
            for i in range(ref.shape[1] // group)
        ]
        for m, ref in enumerate((gate_far, value_far))
    ]
    for copies in raws:
        for copy in copies:
            copy.start()

    has_up, has_down = level < ring - 1, level > 0
    has_after, has_before = sp < members - 1, sp > 0

    barrier = pltpu.get_barrier_semaphore()

    def greet(**device):
        pl.semaphore_signal(barrier, inc=1, device_id=device, device_id_type=MESH)

    greet(tp=mate)
    for turn in (1, 2, 3):
        greet(sp=peer(turn))
    pl.when(has_up)(lambda: greet(sp=sp + TEAM))
    pl.when(has_down)(lambda: greet(sp=sp - TEAM))
    pl.when(has_after)(lambda: greet(sp=sp + 1))
    pl.when(has_before)(lambda: greet(sp=sp - 1))
    others = sum(jnp.where(there, 1, 0) for there in (has_up, has_down, has_after, has_before))
    pl.semaphore_wait(barrier, TEAM + others)

    def begin(copy, there=None):
        if there is None:
            copy.start()
        else:
            pl.when(there)(copy.start)
        sends.append((there, copy))
        return copy

    def arrive(copy, there=None):
        if there is None:
            copy.wait_recv()
        else:
            pl.when(there)(copy.wait_recv)

    halos = [
        begin(
            remote(
                ref.at[pl.ds(length - WINDOW, WINDOW)],
                ext.at[pl.ds(0, WINDOW)],
                halo_s.at[i],
                halo_r.at[i],
                sp=sp + 1,
            ),
            has_after,
        )
        for i, (ref, ext) in enumerate(((k_ref, k_ext), (v_ref, v_ext)))
    ]

    wholes = (gate_all, value_all, down_all)

    def span(m, start, size):
        return wholes[m].at[:, pl.ds(pl.multiple_of(start * wide, wide), size * wide)]

    def piece(m, member):
        if m == 2:
            return down_far.at[pl.ds(pl.multiple_of(member * units, units), units)]
        return hid.at[pl.ds(m * units, units), pl.ds(pl.multiple_of(member * wide, wide), wide)]

    def turn_round(m):
        for i, copy in enumerate(raws[m]):
            copy.wait()
            turned = raw_piece(m, i)[...].T
            at = i * group
            while at < (i + 1) * group:
                member, first = at // units, at % units
                size = min(units - first, (i + 1) * group - at)
                start = at - i * group
                hid[m * units + first : m * units + first + size, member * wide : member * wide + wide] = (
                    turned[start : start + size]
                )
                at += size

    def can_send(side, step):
        return has_up & (level >= step) if side == 0 else has_down & (level + step < ring)

    def can_receive(side, step):
        return level > step if side == 0 else level + step < ring - 1

    def toward(side):
        return sp + TEAM if side == 0 else sp - TEAM

    def first_copy(m, side, q, source=None):
        block = span(m, level * TEAM + q, 1)
        return remote(
            block if source is None else source,
            block,
            first_s.at[m, side, q],
            first_r.at[m, side, q],
            sp=toward(side),
        )

    def next_copy(m, side, step, block, half=None):
        if m == 0:
            part = span(m, block * TEAM, TEAM)
            sems = next_s.at[0, side, step - 1], next_r.at[0, side, step - 1]
        elif m == 1:
            first, size = parts[half]
            part = span(m, block * TEAM, TEAM).at[pl.ds(first, size)]
            sems = next_s.at[1 + half, side, step - 1], next_r.at[1 + half, side, step - 1]
        else:
            first, size = cuts[half]
            part = span(m, block * TEAM + first, size)
            sems = half_s.at[side, step - 1, half], half_r.at[side, step - 1, half]
        return remote(part, part, *sems, sp=toward(side))

    def came(side, step):
        return level - 1 - step if side == 0 else level + 1 + step

    def receive(m, step, half=None):
        for side in range(2):
            there = can_receive(side, step)
            if step == 0:
                members_in = range(TEAM)
                if m == 2:
                    members_in = range(cuts[half][0], sum(cuts[half]))
                for q in members_in:
                    block = span(m, came(side, 0) * TEAM + q, 1)
                    sems = first_s.at[m, side, q], first_r.at[m, side, q]
                    arrive(remote(block, block, *sems, sp=toward(side)), there)
            else:
                arrive(next_copy(m, side, step, came(side, step), half), there)

    def pass_on(m, step, half=None):
        if not (m == 1 and step == 1 and half):
            receive(m, step - 1, half)
        for side in range(2):
            block = level - step if side == 0 else level + step
            begin(next_copy(m, side, step, block, half), can_send(side, step))

    def own_first(m):
        for side in range(2):
            begin(first_copy(m, side, place, piece(m, place)), can_send(side, 0))

    trades, locals_, early = {}, {}, []

    def launch(m):
        mark = len(sends)
        if m < 2:
            turn_round(m)
        trades.update(
            {
                m: {
                turn: begin(
                    remote(
                        piece(m, team_peer(place, turn)),
                        span(m, sp, 1),
                        trade_s.at[m, turn - 1],
                        trade_r.at[m, turn - 1],
                        sp=peer(turn),
                    )
                )
                for turn in (1, 2, 3)
                }
            }
        )
        if m < 2:
            own_first(m)
            early.extend(sends[mark:])
            del sends[mark:]
        copy = pltpu.make_async_copy(piece(m, place), span(m, sp, 1), local_sem.at[m])
        copy.start()
        locals_[m] = copy

    launch(0)
    own_first(2)
    fetch_q = pltpu.make_async_copy(q_far, q_ref, local_sem.at[5])
    fetch_q.start()
    fetch_kv = [
        pltpu.make_async_copy(ref, ext.at[pl.ds(WINDOW, length)], local_sem.at[6 + i])
        for i, (ref, ext) in enumerate(((k_ref, k_ext), (v_ref, v_ext)))
    ]
    for copy in fetch_kv:
        copy.start()
    fetch_ow = pltpu.make_async_copy(ow_far, ow, local_sem.at[3])
    fetch_ow.start()
    fetch_res = pltpu.make_async_copy(res_far, res, local_sem.at[4])
    fetch_res.start()

    def first_rest(m):
        for turn in (1, 2, 3):
            trades[m][turn].wait_recv()
            for side in range(2):
                begin(first_copy(m, side, team_peer(place, turn)), can_send(side, 0))

    def down_rest():
        for q in range(TEAM):
            turn = jnp.abs(place % 2 - q % 2) + 2 * jnp.abs(place // 2 - q // 2)

            @pl.when(turn > 0)
            def _(q=q, turn=turn):
                block = span(2, level * TEAM + q, 1)
                sems = trade_s.at[2, turn - 1], trade_r.at[2, turn - 1]
                remote(block, block, *sems, sp=level * TEAM + q).wait_recv()

            for side in range(2):
                begin(first_copy(2, side, q), can_send(side, 0) & (turn > 0))

    pending = [
        (m, step, part)
        for step in range(1, last + 1)
        for m in range(2)
        for part in (range(len(parts)) if m else (None,))
    ]

    def pass_next(count):
        for m, step, part in pending[:count]:
            pass_on(m, step, part)
        del pending[:count]

    @pl.when(jnp.logical_not(has_before))
    def _():
        k_ext[pl.ds(0, WINDOW)] = jnp.zeros((WINDOW, k_ref.shape[1]), k_ref.dtype)
        v_ext[pl.ds(0, WINDOW)] = jnp.zeros((WINDOW, k_ref.shape[1]), k_ref.dtype)

    for p in range(TEAM):

        @pl.when(place == p)
        def _(p=p):
            for i, ref in enumerate((gate_taps, value_taps)):
                taps[i, : ref.shape[0]] = ref[:, p * units : (p + 1) * units]

    first_rest(0)
    launch(1)
    launch(2)
    for copy in halos:
        arrive(copy, has_before)
    fetch_q.wait()
    for copy in fetch_kv:
        copy.wait()
    heads_kv = k_ref.shape[1] // HD
    grouping = q_ref.shape[1] // k_ref.shape[1]
    row = lax.broadcasted_iota(jnp.int32, (WINDOW, 2 * WINDOW), 0)
    col = lax.broadcasted_iota(jnp.int32, (WINDOW, 2 * WINDOW), 1)
    band = (col <= row + WINDOW) & (col > row)

    for kv in range(heads_kv):

        def block_step(n, carry, kv=kv):
            start = pl.multiple_of(n * WINDOW, WINDOW)
            keys = k_ext[pl.ds(start, 2 * WINDOW), kv * HD : (kv + 1) * HD]
            values = v_ext[pl.ds(start, 2 * WINDOW), kv * HD : (kv + 1) * HD]
            wide_q = q_ref[pl.ds(start, WINDOW), kv * grouping * HD : (kv + 1) * grouping * HD]
            visible = band & (col + (sp * length + start - WINDOW) >= 0)
            stacked = jnp.concatenate(
                [wide_q[:, g * HD : (g + 1) * HD] for g in range(grouping)], axis=0
            )
            scores = lax.dot_general(
                stacked, keys, (((1,), (1,)), ((), ())), preferred_element_type=jnp.float32
            ) * HD ** (-0.5)
            probs = []
            for g in range(grouping):
                sink = sink_ref[kv * grouping + g]
                part = jnp.where(visible, scores[g * WINDOW : (g + 1) * WINDOW], NEG_FILL)
                top = jnp.maximum(jnp.max(part, axis=-1, keepdims=True), sink)
                expo = jnp.exp(part - top)
                whole = jnp.sum(expo, axis=-1, keepdims=True) + jnp.exp(sink - top)
                probs.append((expo / whole).astype(jnp.bfloat16))
            result = jnp.dot(
                jnp.concatenate(probs, axis=0), values, preferred_element_type=jnp.float32
            ).astype(jnp.bfloat16)
            att[pl.ds(start, WINDOW), kv * grouping * HD : (kv + 1) * grouping * HD] = (
                jnp.concatenate(
                    [result[g * WINDOW : (g + 1) * WINDOW] for g in range(grouping)], axis=1
                )
            )
            return carry

        lax.fori_loop(0, length // WINDOW, block_step, 0)
        if kv == 1:
            first_rest(1)

    columns = ow.shape[1]
    tile = min(512, columns)
    fetch_ow.wait()

    def project(rows_start, target):
        def tile_step(t, carry):
            at = pl.multiple_of(t * tile, tile)
            target[:, pl.ds(at, tile)] = jnp.dot(
                att[pl.ds(rows_start, share)],
                ow[:, pl.ds(at, tile)],
                preferred_element_type=jnp.float32,
            ).astype(jnp.bfloat16)
            return carry

        lax.fori_loop(0, columns // tile, tile_step, 0)

    project(pl.multiple_of(mate * share, share), snd)
    pair = begin(remote(snd, rcv, pair_s, pair_r, tp=mate))
    project(pl.multiple_of(tp * share, share), own)
    fetch_res.wait()
    pair.wait_recv()
    band_rows = 32
    rows = length * TEAM
    edge = rows_all.shape[0] - rows

    def row_start(member, core):
        return pl.multiple_of(edge + (member * 2 + core) * share, edge)

    my_rows = row_start(place, tp)

    def norm_step(t, carry):
        at = pl.ds(pl.multiple_of(t * band_rows, band_rows), band_rows)
        proj = own[at].astype(jnp.float32) + rcv[at].astype(jnp.float32)
        middle = res[at].astype(jnp.float32) + proj * row_scale(proj) * ga_ref[...]
        mid[at] = middle
        rows_all[pl.ds(pl.multiple_of(my_rows + t * band_rows, edge), band_rows)] = (
            middle * row_scale(middle) * gb_ref[...]
        ).astype(jnp.bfloat16)
        return carry

    lax.fori_loop(0, share // band_rows, norm_step, 0)

    def slot(member, first=0, size=share):
        start = pl.multiple_of(row_start(member, tp) + first, edge)
        return rows_all.at[pl.ds(start, size)]

    def row_copy(block, i, turn):
        return begin(remote(block, block, rows_s.at[i], rows_r.at[i], sp=peer(turn)))

    def to_mate(block, i):
        return begin(remote(block, block, mate_s.at[i], mate_r.at[i], tp=mate))

    half = share // 2
    mine_rows = slot(place)
    across = [row_copy(mine_rows, 0, 1), row_copy(mine_rows, 1, 2)]
    mates = [to_mate(mine_rows, 0)]
    pass_next(1)
    pass_next(len(parts))
    across[0].wait_recv()
    across.append(row_copy(slot(team_peer(place, 1), 0, half), 2, 2))
    mates.append(to_mate(slot(team_peer(place, 1)), 1))
    across[1].wait_recv()
    across.append(row_copy(slot(team_peer(place, 2), half, half), 3, 1))
    mates.append(to_mate(slot(team_peer(place, 2)), 2))
    pass_next(1)
    across[2].wait_recv()
    across[3].wait_recv()
    mates.append(to_mate(slot(team_peer(place, 3)), 3))
    for copy in mates:
        copy.wait_recv()
    ending = remote(
        rows_all.at[pl.ds(rows, edge)], rows_all.at[pl.ds(0, edge)], edge_s, edge_r, sp=sp + TEAM
    )
    begin(ending, has_up)

    @pl.when(jnp.logical_not(has_down))
    def _():
        rows_all[pl.ds(0, edge)] = jnp.zeros((edge, rows_all.shape[1]), rows_all.dtype)

    pass_next(len(pending))
    arrive(ending, has_down)

    steps = even_parts(rows + edge, 4)
    chunk = (rows + edge) // steps

    def up(m, result, first=0, size=units):
        def up_step(t, carry):
            at = pl.ds(pl.multiple_of(t * chunk, edge), chunk)
            result[at, first : first + size] = rows_by_units(
                rows_all[at], wholes[m][first : first + size]
            ).astype(jnp.bfloat16)
            return carry

        lax.fori_loop(0, steps, up_step, 0)

    receive(0, last)
    locals_[0].wait()
    up(0, gate_up)
    down_rest()
    locals_[1].wait()
    for there, copy in early:
        if there is None:
            copy.wait_send()
        else:
            pl.when(there)(copy.wait_send)
    reach = gate_taps.shape[0] - 1
    conv_rows = 64
    per = share // conv_rows

    def conv_step(t, carry, first_unit, size):
        unit_span = slice(first_unit, first_unit + size)
        at = pl.multiple_of(t * conv_rows, conv_rows)

        def mixed(source, i):
            padded = source[pl.ds(at, conv_rows + edge), unit_span].astype(jnp.float32)
            result = jnp.zeros((conv_rows, size), jnp.float32)
            for k in range(reach + 1):
                first = edge - reach + k
                result = result + taps[i, k : k + 1, unit_span] * padded[first : first + conv_rows]
            return result

        gate = mixed(gate_up, 0)
        value = mixed(value_up, 1)
        group = t // per
        to = (group % 2 * TEAM + group // 2) * share + t % per * conv_rows
        hid[pl.ds(pl.multiple_of(to, conv_rows), conv_rows), unit_span] = (
            gate / (1.0 + jnp.exp(-gate)) * value
        ).astype(jnp.bfloat16)
        return carry

    for i, (first_unit, size) in enumerate(parts):
        receive(1, last, i)
        up(1, value_up, first_unit, size)
        mixing = functools.partial(conv_step, first_unit=first_unit, size=size)
        lax.fori_loop(0, rows // conv_rows, mixing, 0)

    locals_[2].wait()
    pairs = jnp.minimum(level, ring - 1 - level)

    def block_at(i):
        near = jnp.where(i % 2 == 1, level - (i + 1) // 2, level + i // 2)
        return jnp.where(i <= 2 * pairs, near, jnp.where(level < ring // 2, i, ring - 1 - i))

    jobs = [(i, *job) for i in range(ring - 1) for job in ((0, 2, (0,)), (2, 2, (1, 2)))]
    jobs += [(ring - 1, *cut, (i,)) for i, cut in enumerate(cuts)]

    def cols_of(j):
        i, first, size, _ = jobs[j]
        at = pl.multiple_of((block_at(i) * TEAM + first) * wide, size * wide)
        return pl.ds(at, size * wide)

    def width_of(j):
        return slice(0, jobs[j][2] * wide)

    ways = ((1, 2), (2, 1))

    def part_of(way):
        return slice(way * half, (way + 1) * half)

    many = TEAM * share
    half_many = many // 2

    def product(core, cols, store):
        def step(t, carry):
            at = pl.multiple_of(t * half_many, half_many)
            store(
                pl.ds(at, half_many),
                jnp.dot(
                    hid[pl.ds(pl.multiple_of(core * many + at, half_many), half_many)],
                    down_all[:, cols],
                    preferred_element_type=jnp.float32,
                ).astype(jnp.bfloat16),
            )
            return carry

        lax.fori_loop(0, 2, step, 0)

    twos, ones, seconds = {}, {}, {}

    def stage_product(j):
        i, needed = jobs[j][0], jobs[j][3]
        if i >= 1:
            for cut in needed:
                if i <= last:
                    pass_on(2, i, cut)
                else:
                    receive(2, last, cut)
        cols = cols_of(j)

        def away(at, part):
            psnd[j, at, width_of(j)] = part

        def here(at, part):
            mine[j % 2, at, width_of(j)] = part

        product(mate, cols, away)
        there = (j, slice(None), width_of(j))
        sems = sum_s.at[0, j], sum_r.at[0, j]
        twos[j] = begin(remote(psnd.at[*there], prcv.at[*there], *sems, tp=mate))
        product(tp, cols, here)

    def shard(j, way, turn):
        at = pl.ds(pl.multiple_of(team_peer(place, turn) * share + way * half, half), half)
        cols = width_of(j)
        return mine[j % 2, at, cols].astype(jnp.float32) + prcv[j, at, cols].astype(jnp.float32)

    def stage_first(j):
        twos[j].wait_recv()
        cols = width_of(j)
        for way, (one, two) in enumerate(ways):
            h1s[j, way, 0, :, cols] = shard(j, way, one).astype(jnp.bfloat16)
            h1s[j, way, 1, :, cols] = shard(j, way, 3).astype(jnp.bfloat16)
            there = (j, way, slice(None), slice(None), cols)
            sems = sum_s.at[1 + way, j], sum_r.at[1 + way, j]
            ones[j, way] = begin(remote(h1s.at[*there], h1r.at[*there], *sems, sp=peer(one)))
        for way, (one, two) in enumerate(ways):
            total[part_of(way), cols_of(j)] = shard(j, way, 0)
            keep[j % 4, way, :, cols] = shard(j, way, two)

    def stage_second(j):
        cols = width_of(j)
        for way, (one, two) in enumerate(ways):
            ones[j, way].wait_recv()
            h2s[j, way, :, cols] = (
                keep[j % 4, way, :, cols] + h1r[j, way, 1, :, cols].astype(jnp.float32)
            ).astype(jnp.bfloat16)
            there = (j, way, slice(None), cols)
            sems = sum_s.at[3 + way, j], sum_r.at[3 + way, j]
            seconds[j, way] = begin(remote(h2s.at[*there], h2r.at[*there], *sems, sp=peer(two)))
            total[part_of(way), cols_of(j)] += h1r[j, way, 0, :, cols].astype(jnp.float32)

    def stage_last(j):
        cols = width_of(j)
        for way in range(2):
            seconds[j, way].wait_recv()
            total[part_of(way), cols_of(j)] += h2r[j, way, :, cols].astype(jnp.float32)

    stages = ((stage_last, 5), (stage_second, 3), (stage_first, 1), (stage_product, 0))
    for clock in range(len(jobs) + stages[0][1]):
        for stage, late in stages:
            if 0 <= clock - late < len(jobs):
                stage(clock - late)

    def out_step(t, carry):
        at = pl.ds(pl.multiple_of(t * band_rows, band_rows), band_rows)
        block = total[at]
        out_ref[at] = (mid[at] + block * row_scale(block) * gc_ref[...]).astype(out_ref.dtype)
        return carry

    lax.fori_loop(0, share // band_rows, out_step, 0)
    for there, copy in sends:
        if there is None:
            copy.wait_send()
        else:
            pl.when(there)(copy.wait_send)


def on_device_team(
    ring,
    queries,
    key_states,
    value_states,
    sink_logits,
    out_weight,
    residual,
    gain_attn,
    gain_before,
    gain_after,
    gate_weight,
    value_weight,
    gate_taps,
    value_taps,
    down_weight,
):
    length, width = queries.shape[0], residual.shape[1]
    share = residual.shape[0]
    wide, local_units = gate_weight.shape
    units = local_units // TEAM
    rows = length * TEAM
    edge = 16
    vmem = pl.BlockSpec(memory_space=pltpu.VMEM)
    smem = pl.BlockSpec(memory_space=pltpu.SMEM)
    far = pl.BlockSpec(memory_space=pl.ANY)
    dma = pltpu.SemaphoreType.DMA
    bf16, f32 = jnp.bfloat16, jnp.float32
    jobs, group_cols = ring * 2 + 1, TEAM // 2 * wide

    def buffer(*shape, dtype=bf16):
        return pltpu.VMEM(shape, dtype)

    return pl.pallas_call(
        functools.partial(layer_kernel, ring),
        out_shape=jax.ShapeDtypeStruct((share, width), bf16),
        in_specs=[far] * 3 + [smem] + [far] * 2 + [vmem] * 3 + [far] * 3 + [vmem] * 2,
        out_specs=vmem,
        scratch_shapes=[
            buffer(*queries.shape),
            buffer(*out_weight.shape),
            buffer(share, width),
            buffer(share, width, dtype=f32),
            buffer(units, width),
            buffer(units, width),
            buffer(units, width),
            buffer(rows + edge, width),
            buffer(rows + edge, units),
            buffer(rows + edge, units),
            buffer(rows, units),
            buffer(2, 8, units, dtype=f32),
            buffer(length + WINDOW, key_states.shape[1]),
            buffer(length + WINDOW, key_states.shape[1]),
            buffer(*queries.shape),
            buffer(share, width),
            buffer(share, width),
            buffer(share, width),
            buffer(jobs, TEAM * share, group_cols),
            buffer(jobs, TEAM * share, group_cols),
            buffer(2, TEAM * share, group_cols),
            buffer(4, 2, share // 2, group_cols, dtype=f32),
            buffer(jobs, 2, 2, share // 2, group_cols),
            buffer(jobs, 2, 2, share // 2, group_cols),
            buffer(jobs, 2, share // 2, group_cols),
            buffer(jobs, 2, share // 2, group_cols),
            buffer(share, width, dtype=f32),
            dma((2,)),
            dma((2,)),
            dma((3, TEAM - 1)),
            dma((3, TEAM - 1)),
            dma((8,)),
            dma((3, 2, TEAM)),
            dma((3, 2, TEAM)),
            dma((1 + len(unit_parts(units)), 2, ring - 2)),
            dma((1 + len(unit_parts(units)), 2, ring - 2)),
            dma((2, ring - 2, 3)),
            dma((2, ring - 2, 3)),
            dma(()),
            dma(()),
            dma((4,)),
            dma((4,)),
            dma((TEAM,)),
            dma((TEAM,)),
            dma(()),
            dma(()),
            dma((5, jobs)),
            dma((5, jobs)),
            dma((2, local_units // group_cols)),
        ],
        compiler_params=pltpu.CompilerParams(
            collective_id=0, has_side_effects=True, vmem_limit_bytes=VMEM_BYTES
        ),
        name="layer",
    )(
        queries,
        key_states,
        value_states,
        sink_logits,
        out_weight,
        residual,
        gain_attn[None],
        gain_before[None],
        gain_after[None],
        gate_weight,
        value_weight,
        down_weight,
        gate_taps,
        value_taps,
    )


def solution(mesh):
    in_specs = (
        P("sp", "tp"),
        P("sp", "tp"),
        P("sp", "tp"),
        P("tp"),
        P("tp", None),
        P(("sp", "tp"), None),
        P(),
        P(),
        P(),
        P("sp", "tp"),
        P("sp", "tp"),
        P(None, "tp"),
        P(None, "tp"),
        P("tp", "sp"),
    )
    out_specs = P(("sp", "tp"), None)
    members, cores = mesh.shape["sp"], mesh.shape["tp"]
    ring = members // TEAM

    def on_device(*args):
        units, wide = args[13].shape
        teams = cores == 2 and members % TEAM == 0 and ring >= 3
        if teams and units % (TEAM * 16) == 0 and wide % 128 == 0:
            return on_device_team(ring, *args)
        return on_device_plain(*args)

    return jax.shard_map(
        on_device, mesh=mesh, in_specs=in_specs, out_specs=out_specs, check_vma=False
    )
```

```python
import functools

import jax
import jax.numpy as jnp
from jax import lax
from jax.experimental import pallas as pl
from jax.experimental.pallas import tpu as pltpu
from jax.sharding import PartitionSpec as P

HD = 64
WINDOW = 128
TEAM = 4


NEG_FILL = -1e30
MESH = pl.DeviceIdType.MESH
VMEM_BYTES = 63 * 1024 * 1024

def passed_along(block, axis, distance):
    devices = range(lax.axis_size(axis))
    route = [(i - distance, i) for i in devices if i - distance in devices]
    return lax.ppermute(block, axis, route)


def rms_scale(matrix):
    return matrix * lax.rsqrt(jnp.mean(matrix * matrix, axis=-1, keepdims=True) + 1e-06)


def attention_local(queries, key_states, value_states, sink_logits):
    length = queries.shape[0]
    blocks = length // WINDOW
    kv_local = key_states.shape[1] // HD
    grouping = queries.shape[1] // key_states.shape[1]
    earlier_keys, earlier_values = passed_along(
        (key_states[length - WINDOW :], value_states[length - WINDOW :]), "sp", 1
    )
    keys_ext = jnp.concatenate([earlier_keys, key_states], axis=0).reshape(
        blocks + 1, WINDOW, kv_local, HD
    )
    values_ext = jnp.concatenate([earlier_values, value_states], axis=0).reshape(
        blocks + 1, WINDOW, kv_local, HD
    )
    key_blocks = jnp.concatenate([keys_ext[:-1], keys_ext[1:]], axis=1)
    value_blocks = jnp.concatenate([values_ext[:-1], values_ext[1:]], axis=1)
    query_blocks = queries.reshape(blocks, WINDOW, kv_local, grouping, HD)
    offset = lax.axis_index("sp") * length
    qpos = (offset + jnp.arange(length, dtype=jnp.int32)).reshape(blocks, WINDOW)
    kpos = jnp.concatenate([qpos - WINDOW, qpos], axis=1)
    visible = (
        (kpos[:, None, :] <= qpos[:, :, None])
        & (qpos[:, :, None] - kpos[:, None, :] < WINDOW)
        & (kpos[:, None, :] >= 0)
    )
    scores = jnp.einsum(
        "nqhgd,nkhd->nhgqk", query_blocks, key_blocks, preferred_element_type=jnp.float32
    ) * HD ** (-0.5)
    scores = jnp.where(visible[:, None, None], scores, NEG_FILL)
    sink_col = sink_logits.reshape(kv_local, grouping)[None, :, :, None]
    top = jnp.maximum(jnp.max(scores, axis=-1), sink_col)
    expo = jnp.exp(scores - top[..., None])
    total = jnp.sum(expo, axis=-1) + jnp.exp(sink_col - top)
    probs = (expo / total[..., None]).astype(jnp.bfloat16)
    result = jnp.einsum(
        "nhgqk,nkhd->nqhgd", probs, value_blocks, preferred_element_type=jnp.float32
    )
    return result.astype(jnp.bfloat16).reshape(length, queries.shape[1])


def causal_local(upward, earlier, kernel):
    length = upward.shape[0]
    padded = jnp.concatenate([earlier, upward], axis=0).astype(jnp.float32)
    result = jnp.zeros(upward.shape, jnp.float32)
    for tap_index in range(kernel.shape[0]):
        result = result + kernel[tap_index][None, :] * padded[tap_index : tap_index + length]
    return result


def on_device_plain(
    queries,
    key_states,
    value_states,
    sink_logits,
    out_weight,
    residual,
    gain_attn,
    gain_before,
    gain_after,
    gate_weight,
    value_weight,
    gate_taps,
    value_taps,
    down_weight,
):
    length = queries.shape[0]
    attended = attention_local(queries, key_states, value_states, sink_logits)
    selected = attended
    attn_proj = lax.psum_scatter(
        jnp.dot(selected, out_weight, preferred_element_type=jnp.float32).astype(jnp.bfloat16),
        "tp",
        scatter_dimension=0,
        tiled=True,
    ).astype(jnp.float32)
    middle = residual.astype(jnp.float32) + rms_scale(attn_proj) * gain_attn
    normed = (rms_scale(middle) * gain_before).astype(jnp.bfloat16)
    whole_rows = lax.all_gather(normed, "tp", axis=0, tiled=True)
    gate_full, value_full = (
        lax.all_gather(gate_weight, "sp", axis=0, tiled=True),
        lax.all_gather(value_weight, "sp", axis=0, tiled=True),
    )
    gate_up = jnp.dot(whole_rows, gate_full, preferred_element_type=jnp.float32).astype(
        jnp.bfloat16
    )
    value_up = jnp.dot(whole_rows, value_full, preferred_element_type=jnp.float32).astype(
        jnp.bfloat16
    )
    reach = gate_taps.shape[0] - 1
    gate_before, value_before = passed_along(
        (gate_up[length - reach :], value_up[length - reach :]), "sp", 1
    )
    gate_conv = causal_local(gate_up, gate_before, gate_taps)
    value_conv = causal_local(value_up, value_before, value_taps)
    hidden = (jax.nn.silu(gate_conv) * value_conv).astype(jnp.bfloat16)
    down_whole = lax.all_gather(down_weight, "sp", axis=1, tiled=True)
    selected = hidden
    down = lax.psum_scatter(
        jnp.dot(selected, down_whole, preferred_element_type=jnp.float32).astype(jnp.bfloat16),
        "tp",
        scatter_dimension=0,
        tiled=True,
    ).astype(jnp.float32)
    return (middle + rms_scale(down) * gain_after).astype(jnp.bfloat16)


def team_peer(place, turn):
    low, high = place % 2, place // 2
    if turn & 1:
        low = 1 - low
    if turn & 2:
        high = 1 - high
    return high * 2 + low


def remote(src, dst, send, recv, **device):
    return pltpu.make_async_remote_copy(
        src_ref=src, dst_ref=dst, send_sem=send, recv_sem=recv, device_id=device, device_id_type=MESH
    )


def row_scale(block):
    return lax.rsqrt(jnp.mean(block * block, axis=-1, keepdims=True) + 1e-06)


def rows_by_units(rows, weight):
    return lax.dot_general(
        rows, weight, (((1,), (1,)), ((), ())), preferred_element_type=jnp.float32
    )


def even_parts(total, wanted):
    for parts in range(wanted, 0, -1):
        if total % (parts * 16) == 0:
            return parts


def unit_parts(units):
    return [(first, min(256, units - first)) for first in range(0, units, 256)]


def layer_kernel(
    ring,
    q_far,
    k_ref,
    v_ref,
    sink_ref,
    ow_far,
    res_far,
    ga_ref,
    gb_ref,
    gc_ref,
    gate_far,
    value_far,
    down_far,
    gate_taps,
    value_taps,
    out_ref,
    q_ref,
    ow,
    res,
    mid,
    gate_all,
    value_all,
    down_all,
    rows_all,
    gate_up,
    value_up,
    hid,
    taps,
    k_ext,
    v_ext,
    att,
    snd,
    rcv,
    own,
    psnd,
    prcv,
    mine,
    keep,
    h1s,
    h1r,
    h2s,
    h2r,
    total,
    halo_s,
    halo_r,
    trade_s,
    trade_r,
    local_sem,
    first_s,
    first_r,
    next_s,
    next_r,
    half_s,
    half_r,
    pair_s,
    pair_r,
    rows_s,
    rows_r,
    mate_s,
    mate_r,
    edge_s,
    edge_r,
    sum_s,
    sum_r,
    raw_sem,
):
    sp, tp = lax.axis_index("sp"), lax.axis_index("tp")
    members = ring * TEAM
    level, place = sp // TEAM, sp % TEAM
    mate = 1 - tp
    length = q_ref.shape[0]
    share = length // 2
    units = gate_all.shape[0]
    wide, deep = down_far.shape[1], gate_far.shape[0]
    last = ring - 2
    parts = unit_parts(units)
    cuts = ((0, 2), (2, 1), (3, 1))
    sends = []

    def peer(turn):
        return level * TEAM + team_peer(place, turn)

    group = psnd.shape[2]
    stacked_raw = psnd.shape[1] // deep

    def raw_piece(m, i):
        at = pl.ds(i % stacked_raw * deep, deep)
        return psnd.at[2 * m + i // stacked_raw, at]

    raws = [
        [
            pltpu.make_async_copy(
                ref.at[:, pl.ds(i * group, group)], raw_piece(m, i), raw_sem.at[m, i]
            )
            for i in range(ref.shape[1] // group)
        ]
        for m, ref in enumerate((gate_far, value_far))
    ]
    for copies in raws:
        for copy in copies:
            copy.start()

    has_up, has_down = level < ring - 1, level > 0
    has_after, has_before = sp < members - 1, sp > 0

    barrier = pltpu.get_barrier_semaphore()

    def greet(**device):
        pl.semaphore_signal(barrier, inc=1, device_id=device, device_id_type=MESH)

    greet(tp=mate)
    for turn in (1, 2, 3):
        greet(sp=peer(turn))
    pl.when(has_up)(lambda: greet(sp=sp + TEAM))
    pl.when(has_down)(lambda: greet(sp=sp - TEAM))
    pl.when(has_after)(lambda: greet(sp=sp + 1))
    pl.when(has_before)(lambda: greet(sp=sp - 1))
    others = sum(jnp.where(there, 1, 0) for there in (has_up, has_down, has_after, has_before))
    pl.semaphore_wait(barrier, TEAM + others)

    def begin(copy, there=None):
        if there is None:
            copy.start()
        else:
            pl.when(there)(copy.start)
        sends.append((there, copy))
        return copy

    def arrive(copy, there=None):
        if there is None:
            copy.wait_recv()
        else:
            pl.when(there)(copy.wait_recv)

    halos = [
        begin(
            remote(
                ref.at[pl.ds(length - WINDOW, WINDOW)],
                ext.at[pl.ds(0, WINDOW)],
                halo_s.at[i],
                halo_r.at[i],
                sp=sp + 1,
            ),
            has_after,
        )
        for i, (ref, ext) in enumerate(((k_ref, k_ext), (v_ref, v_ext)))
    ]

    wholes = (gate_all, value_all, down_all)

    def span(m, start, size):
        return wholes[m].at[:, pl.ds(pl.multiple_of(start * wide, wide), size * wide)]

    def piece(m, member):
        if m == 2:
            return down_far.at[pl.ds(pl.multiple_of(member * units, units), units)]
        return hid.at[pl.ds(m * units, units), pl.ds(pl.multiple_of(member * wide, wide), wide)]

    def turn_round(m):
        for i, copy in enumerate(raws[m]):
            copy.wait()
            turned = raw_piece(m, i)[...].T
            at = i * group
            while at < (i + 1) * group:
                member, first = at // units, at % units
                size = min(units - first, (i + 1) * group - at)
                start = at - i * group
                hid[m * units + first : m * units + first + size, member * wide : member * wide + wide] = (
                    turned[start : start + size]
                )
                at += size

    def can_send(side, step):
        return has_up & (level >= step) if side == 0 else has_down & (level + step < ring)

    def can_receive(side, step):
        return level > step if side == 0 else level + step < ring - 1

    def toward(side):
        return sp + TEAM if side == 0 else sp - TEAM

    def first_copy(m, side, q, source=None):
        block = span(m, level * TEAM + q, 1)
        return remote(
            block if source is None else source,
            block,
            first_s.at[m, side, q],
            first_r.at[m, side, q],
            sp=toward(side),
        )

    def next_copy(m, side, step, block, half=None):
        if m == 0:
            part = span(m, block * TEAM, TEAM)
            sems = next_s.at[0, side, step - 1], next_r.at[0, side, step - 1]
        elif m == 1:
            first, size = parts[half]
            part = span(m, block * TEAM, TEAM).at[pl.ds(first, size)]
            sems = next_s.at[1 + half, side, step - 1], next_r.at[1 + half, side, step - 1]
        else:
            first, size = cuts[half]
            part = span(m, block * TEAM + first, size)
            sems = half_s.at[side, step - 1, half], half_r.at[side, step - 1, half]
        return remote(part, part, *sems, sp=toward(side))

    def came(side, step):
        return level - 1 - step if side == 0 else level + 1 + step

    def receive(m, step, half=None):
        for side in range(2):
            there = can_receive(side, step)
            if step == 0:
                members_in = range(TEAM)
                if m == 2:
                    members_in = range(cuts[half][0], sum(cuts[half]))
                for q in members_in:
                    block = span(m, came(side, 0) * TEAM + q, 1)
                    sems = first_s.at[m, side, q], first_r.at[m, side, q]
                    arrive(remote(block, block, *sems, sp=toward(side)), there)
            else:
                arrive(next_copy(m, side, step, came(side, step), half), there)

    def pass_on(m, step, half=None):
        if not (m == 1 and step == 1 and half):
            receive(m, step - 1, half)
        for side in range(2):
            block = level - step if side == 0 else level + step
            begin(next_copy(m, side, step, block, half), can_send(side, step))

    def own_first(m):
        for side in range(2):
            begin(first_copy(m, side, place, piece(m, place)), can_send(side, 0))

    trades, locals_, early = {}, {}, []

    def launch(m):
        mark = len(sends)
        if m < 2:
            turn_round(m)
        trades.update(
            {
                m: {
                turn: begin(
                    remote(
                        piece(m, team_peer(place, turn)),
                        span(m, sp, 1),
                        trade_s.at[m, turn - 1],
                        trade_r.at[m, turn - 1],
                        sp=peer(turn),
                    )
                )
                for turn in (1, 2, 3)
                }
            }
        )
        if m < 2:
            own_first(m)
            early.extend(sends[mark:])
            del sends[mark:]
        copy = pltpu.make_async_copy(piece(m, place), span(m, sp, 1), local_sem.at[m])
        copy.start()
        locals_[m] = copy

    launch(0)
    own_first(2)
    fetch_q = pltpu.make_async_copy(q_far, q_ref, local_sem.at[5])
    fetch_q.start()
    fetch_kv = [
        pltpu.make_async_copy(ref, ext.at[pl.ds(WINDOW, length)], local_sem.at[6 + i])
        for i, (ref, ext) in enumerate(((k_ref, k_ext), (v_ref, v_ext)))
    ]
    for copy in fetch_kv:
        copy.start()
    fetch_ow = pltpu.make_async_copy(ow_far, ow, local_sem.at[3])
    fetch_ow.start()
    fetch_res = pltpu.make_async_copy(res_far, res, local_sem.at[4])
    fetch_res.start()

    def first_rest(m):
        for turn in (1, 2, 3):
            trades[m][turn].wait_recv()
            for side in range(2):
                begin(first_copy(m, side, team_peer(place, turn)), can_send(side, 0))

    def down_rest():
        for q in range(TEAM):
            turn = jnp.abs(place % 2 - q % 2) + 2 * jnp.abs(place // 2 - q // 2)

            @pl.when(turn > 0)
            def _(q=q, turn=turn):
                block = span(2, level * TEAM + q, 1)
                sems = trade_s.at[2, turn - 1], trade_r.at[2, turn - 1]
                remote(block, block, *sems, sp=level * TEAM + q).wait_recv()

            for side in range(2):
                begin(first_copy(2, side, q), can_send(side, 0) & (turn > 0))

    pending = [
        (m, step, part)
        for step in range(1, last + 1)
        for m in range(2)
        for part in (range(len(parts)) if m else (None,))
    ]

    def pass_next(count):
        for m, step, part in pending[:count]:
            pass_on(m, step, part)
        del pending[:count]

    @pl.when(jnp.logical_not(has_before))
    def _():
        k_ext[pl.ds(0, WINDOW)] = jnp.zeros((WINDOW, k_ref.shape[1]), k_ref.dtype)
        v_ext[pl.ds(0, WINDOW)] = jnp.zeros((WINDOW, k_ref.shape[1]), k_ref.dtype)

    for p in range(TEAM):

        @pl.when(place == p)
        def _(p=p):
            for i, ref in enumerate((gate_taps, value_taps)):
                taps[i, : ref.shape[0]] = ref[:, p * units : (p + 1) * units]

    launch(1)
    first_rest(0)
    launch(2)
    for copy in halos:
        arrive(copy, has_before)
    fetch_q.wait()
    for copy in fetch_kv:
        copy.wait()
    heads_kv = k_ref.shape[1] // HD
    grouping = q_ref.shape[1] // k_ref.shape[1]
    row = lax.broadcasted_iota(jnp.int32, (WINDOW, 2 * WINDOW), 0)
    col = lax.broadcasted_iota(jnp.int32, (WINDOW, 2 * WINDOW), 1)
    band = (col <= row + WINDOW) & (col > row)

    for kv in range(heads_kv):

        def block_step(n, carry, kv=kv):
            start = pl.multiple_of(n * WINDOW, WINDOW)
            keys = k_ext[pl.ds(start, 2 * WINDOW), kv * HD : (kv + 1) * HD]
            values = v_ext[pl.ds(start, 2 * WINDOW), kv * HD : (kv + 1) * HD]
            wide_q = q_ref[pl.ds(start, WINDOW), kv * grouping * HD : (kv + 1) * grouping * HD]
            visible = band & (col + (sp * length + start - WINDOW) >= 0)
            stacked = jnp.concatenate(
                [wide_q[:, g * HD : (g + 1) * HD] for g in range(grouping)], axis=0
            )
            scores = lax.dot_general(
                stacked, keys, (((1,), (1,)), ((), ())), preferred_element_type=jnp.float32
            ) * HD ** (-0.5)
            probs = []
            for g in range(grouping):
                sink = sink_ref[kv * grouping + g]
                part = jnp.where(visible, scores[g * WINDOW : (g + 1) * WINDOW], NEG_FILL)
                top = jnp.maximum(jnp.max(part, axis=-1, keepdims=True), sink)
                expo = jnp.exp(part - top)
                whole = jnp.sum(expo, axis=-1, keepdims=True) + jnp.exp(sink - top)
                probs.append((expo / whole).astype(jnp.bfloat16))
            result = jnp.dot(
                jnp.concatenate(probs, axis=0), values, preferred_element_type=jnp.float32
            ).astype(jnp.bfloat16)
            att[pl.ds(start, WINDOW), kv * grouping * HD : (kv + 1) * grouping * HD] = (
                jnp.concatenate(
                    [result[g * WINDOW : (g + 1) * WINDOW] for g in range(grouping)], axis=1
                )
            )
            return carry

        lax.fori_loop(0, length // WINDOW, block_step, 0)
        if kv == 1:
            first_rest(1)

    columns = ow.shape[1]
    tile = min(512, columns)
    fetch_ow.wait()

    def project(rows_start, target):
        def tile_step(t, carry):
            at = pl.multiple_of(t * tile, tile)
            target[:, pl.ds(at, tile)] = jnp.dot(
                att[pl.ds(rows_start, share)],
                ow[:, pl.ds(at, tile)],
                preferred_element_type=jnp.float32,
            ).astype(jnp.bfloat16)
            return carry

        lax.fori_loop(0, columns // tile, tile_step, 0)

    project(pl.multiple_of(mate * share, share), snd)
    pair = begin(remote(snd, rcv, pair_s, pair_r, tp=mate))
    project(pl.multiple_of(tp * share, share), own)
    fetch_res.wait()
    pair.wait_recv()
    band_rows = 32
    rows = length * TEAM
    edge = rows_all.shape[0] - rows

    def row_start(member, core):
        return pl.multiple_of(edge + (member * 2 + core) * share, edge)

    my_rows = row_start(place, tp)

    def norm_step(t, carry):
        at = pl.ds(pl.multiple_of(t * band_rows, band_rows), band_rows)
        proj = own[at].astype(jnp.float32) + rcv[at].astype(jnp.float32)
        middle = res[at].astype(jnp.float32) + proj * row_scale(proj) * ga_ref[...]
        mid[at] = middle
        rows_all[pl.ds(pl.multiple_of(my_rows + t * band_rows, edge), band_rows)] = (
            middle * row_scale(middle) * gb_ref[...]
        ).astype(jnp.bfloat16)
        return carry

    lax.fori_loop(0, share // band_rows, norm_step, 0)

    def slot(member, first=0, size=share):
        start = pl.multiple_of(row_start(member, tp) + first, edge)
        return rows_all.at[pl.ds(start, size)]

    def row_copy(block, i, turn):
        return begin(remote(block, block, rows_s.at[i], rows_r.at[i], sp=peer(turn)))

    def to_mate(block, i):
        return begin(remote(block, block, mate_s.at[i], mate_r.at[i], tp=mate))

    half = share // 2
    mine_rows = slot(place)
    across = [row_copy(mine_rows, 0, 1), row_copy(mine_rows, 1, 2)]
    mates = [to_mate(mine_rows, 0)]
    pass_next(1)
    pass_next(len(parts))
    across[0].wait_recv()
    across.append(row_copy(slot(team_peer(place, 1), 0, half), 2, 2))
    mates.append(to_mate(slot(team_peer(place, 1)), 1))
    across[1].wait_recv()
    across.append(row_copy(slot(team_peer(place, 2), half, half), 3, 1))
    mates.append(to_mate(slot(team_peer(place, 2)), 2))
    pass_next(1)
    across[2].wait_recv()
    across[3].wait_recv()
    mates.append(to_mate(slot(team_peer(place, 3)), 3))
    for copy in mates:
        copy.wait_recv()
    ending = remote(
        rows_all.at[pl.ds(rows, edge)], rows_all.at[pl.ds(0, edge)], edge_s, edge_r, sp=sp + TEAM
    )
    begin(ending, has_up)

    @pl.when(jnp.logical_not(has_down))
    def _():
        rows_all[pl.ds(0, edge)] = jnp.zeros((edge, rows_all.shape[1]), rows_all.dtype)

    pass_next(len(pending))
    arrive(ending, has_down)

    steps = even_parts(rows + edge, 4)
    chunk = (rows + edge) // steps

    def up(m, result, first=0, size=units):
        def up_step(t, carry):
            at = pl.ds(pl.multiple_of(t * chunk, edge), chunk)
            result[at, first : first + size] = rows_by_units(
                rows_all[at], wholes[m][first : first + size]
            ).astype(jnp.bfloat16)
            return carry

        lax.fori_loop(0, steps, up_step, 0)

    receive(0, last)
    locals_[0].wait()
    down_rest()
    up(0, gate_up)
    locals_[1].wait()
    for there, copy in early:
        if there is None:
            copy.wait_send()
        else:
            pl.when(there)(copy.wait_send)
    reach = gate_taps.shape[0] - 1
    conv_rows = 64
    per = share // conv_rows

    def conv_step(t, carry, first_unit, size):
        unit_span = slice(first_unit, first_unit + size)
        at = pl.multiple_of(t * conv_rows, conv_rows)

        def mixed(source, i):
            padded = source[pl.ds(at, conv_rows + edge), unit_span].astype(jnp.float32)
            result = jnp.zeros((conv_rows, size), jnp.float32)
            for k in range(reach + 1):
                first = edge - reach + k
                result = result + taps[i, k : k + 1, unit_span] * padded[first : first + conv_rows]
            return result

        gate = mixed(gate_up, 0)
        value = mixed(value_up, 1)
        group = t // per
        to = (group % 2 * TEAM + group // 2) * share + t % per * conv_rows
        hid[pl.ds(pl.multiple_of(to, conv_rows), conv_rows), unit_span] = (
            gate / (1.0 + jnp.exp(-gate)) * value
        ).astype(jnp.bfloat16)
        return carry

    for i, (first_unit, size) in enumerate(parts):
        receive(1, last, i)
        up(1, value_up, first_unit, size)
        mixing = functools.partial(conv_step, first_unit=first_unit, size=size)
        lax.fori_loop(0, rows // conv_rows, mixing, 0)

    locals_[2].wait()
    pairs = jnp.minimum(level, ring - 1 - level)

    def block_at(i):
        near = jnp.where(i % 2 == 1, level - (i + 1) // 2, level + i // 2)
        return jnp.where(i <= 2 * pairs, near, jnp.where(level < ring // 2, i, ring - 1 - i))

    jobs = [(i, *job) for i in range(ring - 1) for job in ((0, 2, (0,)), (2, 2, (1, 2)))]
    jobs += [(ring - 1, *cut, (i,)) for i, cut in enumerate(cuts)]

    def cols_of(j):
        i, first, size, _ = jobs[j]
        at = pl.multiple_of((block_at(i) * TEAM + first) * wide, size * wide)
        return pl.ds(at, size * wide)

    def width_of(j):
        return slice(0, jobs[j][2] * wide)

    ways = ((1, 2), (2, 1))

    def part_of(way):
        return slice(way * half, (way + 1) * half)

    many = TEAM * share
    half_many = many // 2

    def product(core, cols, store):
        def step(t, carry):
            at = pl.multiple_of(t * half_many, half_many)
            store(
                pl.ds(at, half_many),
                jnp.dot(
                    hid[pl.ds(pl.multiple_of(core * many + at, half_many), half_many)],
                    down_all[:, cols],
                    preferred_element_type=jnp.float32,
                ).astype(jnp.bfloat16),
            )
            return carry

        lax.fori_loop(0, 2, step, 0)

    twos, ones, seconds = {}, {}, {}

    def stage_product(j):
        i, needed = jobs[j][0], jobs[j][3]
        if i >= 1:
            for cut in needed:
                if i <= last:
                    pass_on(2, i, cut)
                else:
                    receive(2, last, cut)
        cols = cols_of(j)

        def away(at, part):
            psnd[j, at, width_of(j)] = part

        def here(at, part):
            mine[j % 2, at, width_of(j)] = part

        product(mate, cols, away)
        there = (j, slice(None), width_of(j))
        sems = sum_s.at[0, j], sum_r.at[0, j]
        twos[j] = begin(remote(psnd.at[*there], prcv.at[*there], *sems, tp=mate))
        product(tp, cols, here)

    def shard(j, way, turn):
        at = pl.ds(pl.multiple_of(team_peer(place, turn) * share + way * half, half), half)
        cols = width_of(j)
        return mine[j % 2, at, cols].astype(jnp.float32) + prcv[j, at, cols].astype(jnp.float32)

    def stage_first(j):
        twos[j].wait_recv()
        cols = width_of(j)
        for way, (one, two) in enumerate(ways):
            h1s[j, way, 0, :, cols] = shard(j, way, one).astype(jnp.bfloat16)
            h1s[j, way, 1, :, cols] = shard(j, way, 3).astype(jnp.bfloat16)
            there = (j, way, slice(None), slice(None), cols)
            sems = sum_s.at[1 + way, j], sum_r.at[1 + way, j]
            ones[j, way] = begin(remote(h1s.at[*there], h1r.at[*there], *sems, sp=peer(one)))
        for way, (one, two) in enumerate(ways):
            total[part_of(way), cols_of(j)] = shard(j, way, 0)
            keep[j % 4, way, :, cols] = shard(j, way, two)

    def stage_second(j):
        cols = width_of(j)
        for way, (one, two) in enumerate(ways):
            ones[j, way].wait_recv()
            h2s[j, way, :, cols] = (
                keep[j % 4, way, :, cols] + h1r[j, way, 1, :, cols].astype(jnp.float32)
            ).astype(jnp.bfloat16)
            there = (j, way, slice(None), cols)
            sems = sum_s.at[3 + way, j], sum_r.at[3 + way, j]
            seconds[j, way] = begin(remote(h2s.at[*there], h2r.at[*there], *sems, sp=peer(two)))
            total[part_of(way), cols_of(j)] += h1r[j, way, 0, :, cols].astype(jnp.float32)

    def stage_last(j):
        cols = width_of(j)
        for way in range(2):
            seconds[j, way].wait_recv()
            total[part_of(way), cols_of(j)] += h2r[j, way, :, cols].astype(jnp.float32)

    stages = ((stage_last, 5), (stage_second, 3), (stage_first, 1), (stage_product, 0))
    for clock in range(len(jobs) + stages[0][1]):
        for stage, late in stages:
            if 0 <= clock - late < len(jobs):
                stage(clock - late)

    def out_step(t, carry):
        at = pl.ds(pl.multiple_of(t * band_rows, band_rows), band_rows)
        block = total[at]
        out_ref[at] = (mid[at] + block * row_scale(block) * gc_ref[...]).astype(out_ref.dtype)
        return carry

    lax.fori_loop(0, share // band_rows, out_step, 0)
    for there, copy in sends:
        if there is None:
            copy.wait_send()
        else:
            pl.when(there)(copy.wait_send)


def on_device_team(
    ring,
    queries,
    key_states,
    value_states,
    sink_logits,
    out_weight,
    residual,
    gain_attn,
    gain_before,
    gain_after,
    gate_weight,
    value_weight,
    gate_taps,
    value_taps,
    down_weight,
):
    length, width = queries.shape[0], residual.shape[1]
    share = residual.shape[0]
    wide, local_units = gate_weight.shape
    units = local_units // TEAM
    rows = length * TEAM
    edge = 16
    vmem = pl.BlockSpec(memory_space=pltpu.VMEM)
    smem = pl.BlockSpec(memory_space=pltpu.SMEM)
    far = pl.BlockSpec(memory_space=pl.ANY)
    dma = pltpu.SemaphoreType.DMA
    bf16, f32 = jnp.bfloat16, jnp.float32
    jobs, group_cols = ring * 2 + 1, TEAM // 2 * wide

    def buffer(*shape, dtype=bf16):
        return pltpu.VMEM(shape, dtype)

    return pl.pallas_call(
        functools.partial(layer_kernel, ring),
        out_shape=jax.ShapeDtypeStruct((share, width), bf16),
        in_specs=[far] * 3 + [smem] + [far] * 2 + [vmem] * 3 + [far] * 3 + [vmem] * 2,
        out_specs=vmem,
        scratch_shapes=[
            buffer(*queries.shape),
            buffer(*out_weight.shape),
            buffer(share, width),
            buffer(share, width, dtype=f32),
            buffer(units, width),
            buffer(units, width),
            buffer(units, width),
            buffer(rows + edge, width),
            buffer(rows + edge, units),
            buffer(rows + edge, units),
            buffer(rows, units),
            buffer(2, 8, units, dtype=f32),
            buffer(length + WINDOW, key_states.shape[1]),
            buffer(length + WINDOW, key_states.shape[1]),
            buffer(*queries.shape),
            buffer(share, width),
            buffer(share, width),
            buffer(share, width),
            buffer(jobs, TEAM * share, group_cols),
            buffer(jobs, TEAM * share, group_cols),
            buffer(2, TEAM * share, group_cols),
            buffer(4, 2, share // 2, group_cols, dtype=f32),
            buffer(jobs, 2, 2, share // 2, group_cols),
            buffer(jobs, 2, 2, share // 2, group_cols),
            buffer(jobs, 2, share // 2, group_cols),
            buffer(jobs, 2, share // 2, group_cols),
            buffer(share, width, dtype=f32),
            dma((2,)),
            dma((2,)),
            dma((3, TEAM - 1)),
            dma((3, TEAM - 1)),
            dma((8,)),
            dma((3, 2, TEAM)),
            dma((3, 2, TEAM)),
            dma((1 + len(unit_parts(units)), 2, ring - 2)),
            dma((1 + len(unit_parts(units)), 2, ring - 2)),
            dma((2, ring - 2, 3)),
            dma((2, ring - 2, 3)),
            dma(()),
            dma(()),
            dma((4,)),
            dma((4,)),
            dma((TEAM,)),
            dma((TEAM,)),
            dma(()),
            dma(()),
            dma((5, jobs)),
            dma((5, jobs)),
            dma((2, local_units // group_cols)),
        ],
        compiler_params=pltpu.CompilerParams(
            collective_id=0, has_side_effects=True, vmem_limit_bytes=VMEM_BYTES
        ),
        name="layer",
    )(
        queries,
        key_states,
        value_states,
        sink_logits,
        out_weight,
        residual,
        gain_attn[None],
        gain_before[None],
        gain_after[None],
        gate_weight,
        value_weight,
        down_weight,
        gate_taps,
        value_taps,
    )


def solution(mesh):
    in_specs = (
        P("sp", "tp"),
        P("sp", "tp"),
        P("sp", "tp"),
        P("tp"),
        P("tp", None),
        P(("sp", "tp"), None),
        P(),
        P(),
        P(),
        P("sp", "tp"),
        P("sp", "tp"),
        P(None, "tp"),
        P(None, "tp"),
        P("tp", "sp"),
    )
    out_specs = P(("sp", "tp"), None)
    members, cores = mesh.shape["sp"], mesh.shape["tp"]
    ring = members // TEAM

    def on_device(*args):
        units, wide = args[13].shape
        teams = cores == 2 and members % TEAM == 0 and ring >= 3
        if teams and units % (TEAM * 16) == 0 and wide % 128 == 0:
            return on_device_team(ring, *args)
        return on_device_plain(*args)

    return jax.shard_map(
        on_device, mesh=mesh, in_specs=in_specs, out_specs=out_specs, check_vma=False
    )
```
